32 devices in a mesh: sp: 8 (over z, core), tp: 4 (over y, x).
Axes of the slice: x: 2, y: 2, z: 4, core: 2. Of those that a mesh axis runs over, the one named last changes fastest.
Arguments:
- cotangent: bfloat16 [1024, 2048], P('sp'), may hold values from -6 to 6
- normed: bfloat16 [1024, 2048], P('sp'), may hold values from -6 to 6
- inverse_root_mean_square: float32 [1024], P('sp'), may hold values from 0.5 to 2
- expert_norm_scale: float32 [2048], replicated, may hold values from 0.1 to 1.9
- routes: int32 [1024, 2], P('sp'), may hold values from 0 to 7, all different within a row; in each aligned block of 128 rows (0 to 127, 128 to 255, ...) at most 64 rows name the same one
- route_probability_weight: float32 [1024, 2], P('sp'), may hold values from 0.2 to 1
- gate_weight: bfloat16 [8, 2048, 2048], P('sp', None, 'tp'), may hold values from -0.125 to 0.125
- up_weight: bfloat16 [8, 2048, 2048], P('sp', None, 'tp'), may hold values from -0.125 to 0.125
- down_weight: bfloat16 [8, 2048, 2048], P('sp', 'tp'), may hold values from -0.125 to 0.125
- recurrence_input: bfloat16 [1024, 1024], P('sp', 'tp'), may hold values from -6 to 6
- recurrence_gate_logits: bfloat16 [1024, 1024], P('sp', 'tp'), may hold values from -6 to 6
- input_gate_logits: bfloat16 [1024, 1024], P('sp', 'tp'), may hold values from -6 to 6
- channel_decay_weight: float32 [1024], P('tp'), may hold values from 3 to 20
- extra_log_decay: float32 [1024, 1024], P('sp', 'tp'), may hold values from -1 to 0
- output_matrix: bfloat16 [2048, 1024], P(None, 'tp'), may hold values from -0.1875 to 0.1875
Outputs:
- grad_gate: bfloat16 [8, 2048, 2048], P('sp', None, 'tp')
- grad_up: bfloat16 [8, 2048, 2048], P('sp', None, 'tp')
- grad_down: bfloat16 [8, 2048, 2048], P('sp', 'tp')
- grad_out_weight: float32 [2048, 1024], P('sp', 'tp')
- grad_rec_input: float32 [1024, 1024], P('sp', 'tp')
- grad_decay_gate: float32 [1024, 1024], P('sp', 'tp')
- grad_input_gate: float32 [1024, 1024], P('sp', 'tp')
The draws below stay inside these ranges and needn't reach their ends.
Inputs may be any that keep to these rules, and one draw needn't show every extreme that they name: `routes`: each row names 2 different experts; among the rows of one device no expert is named more than 64 times.
All inputs are finite; a program needn't handle non-finite values.
Results may differ from the reference program's by a relative error of at most 0.025.
Values may be sent and summed in bfloat16 or wider, within the bound.
A program may use at most 64 MiB of HBM per device.

```python
import math
import jax
import jax.numpy as jnp
import numpy as np
from jax import lax

D = 2048
C = 1024
FF = 2048
TOPK = 2
TOK_DEV = 128
EXPERTS = 8
CAP = 64
TOKENS = 1024
N_SP = 8
N_TP = 4


def draw_channel_decay_weight(key, part):
    first, second, third = jax.random.split(key, 3)
    share = 0.5
    quick = jax.random.uniform(first, (C,), jnp.float32) < share
    slow_rate = jnp.exp(jax.random.uniform(second, (C,), jnp.float32, jnp.log(0.02), jnp.log(0.12))) / TOKENS
    quick_rate = jnp.exp(jax.random.uniform(third, (C,), jnp.float32, jnp.log(0.005), jnp.log(0.02)))
    rate = jnp.where(quick, quick_rate, slow_rate)
    return (-jnp.log(jnp.expm1(rate))).astype(jnp.float32)


def draw_extra_log_decay(key, part):
    first, second = jax.random.split(key, 2)
    places = jax.random.randint(first, (3,), 0, TOKENS)
    struck = jnp.any(jnp.arange(TOKENS)[:, None] == places[None, :], axis=1)
    depth = jnp.log(jax.random.uniform(second, (TOKENS, C), jnp.float32, 0.65, 0.85))
    return jnp.where(struck[:, None], depth, 0.0).astype(jnp.float32)


def draw_recurrence_gate_logits(key, part):
    first, second = jax.random.split(key, 2)
    blocks = TOKENS // TOK_DEV
    offset = jax.random.uniform(first, (blocks,), jnp.float32, -1.0, 1.0)
    noise = jnp.clip(jax.random.normal(second, (TOKENS, C), jnp.float32) * 0.7, -3.5, 3.5)
    return (noise + jnp.repeat(offset, TOK_DEV)[:, None]).astype(jnp.bfloat16)


def raised(drawn, own_key, source, target, shards_of, factor):
    owner, partner = [(jnp.arange(drawn.shape[position]) // (drawn.shape[position] // shards_of)).reshape([-1 if axis == position else 1 for axis in range(drawn.ndim)]) for position in (source, target)]
    chosen = jax.random.permutation(own_key, shards_of)[partner]
    strong = (owner == chosen) | (owner == (partner + shards_of // 2) % shards_of)
    return jnp.where(strong, factor * drawn, drawn)


def shard_levels(stream_key, extent, cuts, least, largest):
    factor_of, own = 1.0, jax.random.fold_in(stream_key, 6)
    for axis_at, parts in cuts:
        draws = jnp.exp(jax.random.uniform(jax.random.fold_in(own, axis_at), (parts,), jnp.float32, least / len(cuts), largest / len(cuts)))
        factor_of = factor_of * jnp.repeat(draws, extent[axis_at] // parts).reshape([-1 if axis == axis_at else 1 for axis in range(len(extent))])
    return factor_of


def routed_block(key, own, number, rows, number_of, top, most, lean):
    order = jax.random.permutation(key, number_of)
    packed, ordinary = shares(number_of, rows * top, most, lean, True), shares(number_of, rows * top, most, lean, False)
    places = jnp.arange(number_of)

    def named(tallies, rotation):
        used = int((tallies > 0).sum())
        fixed = max(1, used // 4)
        moved = fixed + (places - fixed + rotation * (used - fixed)) % max(1, number_of - fixed)
        return jnp.zeros((number_of,), jnp.int32).at[order[jnp.where(places < fixed, places, moved)]].set(jnp.asarray(tallies, jnp.int32))

    tallies = jnp.where(number % 4 == 0, named(packed, number // 4), named(ordinary, number - number // 4 - 1))
    mixed = jax.random.permutation(jax.random.fold_in(own, 3), number_of)
    source_of, receiver = mixed[0:number_of // 2 * 2:2], mixed[1:number_of // 2 * 2:2]
    room = jnp.minimum(tallies[source_of] - 1, most - tallies[receiver]) // 2
    room = jnp.where((source_of == order[0]) | (receiver == order[0]) | (tallies[receiver] == 0), 0, jnp.maximum(room, 0))
    moved = jax.random.randint(jax.random.fold_in(own, 4), (number_of // 2,), 0, 1 << 20) % (room + 1)
    tallies = tallies.at[source_of].add(-moved).at[receiver].add(moved)
    items = jnp.searchsorted(jnp.cumsum(tallies), jnp.arange(rows * top), side="right").astype(jnp.int32)
    listing = items.reshape(top, rows).T
    listing = listing[jax.random.permutation(jax.random.fold_in(own, 1), rows)]
    rotation = jax.random.randint(jax.random.fold_in(own, 2), (rows, 1), 0, top)
    return jnp.take_along_axis(listing, (jnp.arange(top)[None, :] + rotation) % top, axis=1)


def shares(amount, total, most, lean, full):
    loads = [(1 << 20) // math.isqrt(grade ** lean) + 1 for grade in range(1, amount + 1)]
    largest = most if full else min(most, max(-(-total // amount), total * loads[0] // sum(loads)))
    least = 1 if total - largest >= amount - 1 else 0
    holding, rest = [largest] + [least] * (amount - 1), total - largest - least * (amount - 1)
    while rest > 0:
        candidates = [i for i in range(1, amount) if holding[i] < largest] or [i for i in range(1, amount) if holding[i] < most]
        pool, remaining = sum([loads[i] for i in candidates]), rest
        for i in candidates:
            addition = min(most - holding[i], max(1, remaining * loads[i] // pool), rest)
            holding[i] = holding[i] + addition
            rest = rest - addition
    return np.array(holding)


def gaussian(rng, shape, width, reach, cuts=(), kind=jnp.bfloat16):
    loudness = shard_levels(rng, shape, cuts, -0.22, 0.18) if cuts else 1.0
    values = jax.random.normal(rng, shape, jnp.float32) * width * loudness
    return jnp.minimum(jnp.maximum(values, -reach), reach).astype(kind)


def gaussian_with(own_key, extent, scale, bound, shards, heavy, kind=jnp.bfloat16):
    entries = scale * jax.random.normal(own_key, extent, jnp.float32)
    if shards:
        entries = entries * shard_levels(own_key, extent, shards, -0.22, 0.18)
    return jnp.clip(raised(entries, jax.random.fold_in(own_key, 3), *heavy), -bound, bound).astype(kind)


def setup_inputs(seed: int = 0) -> dict:
    key_list = jax.random.split(jax.random.key(seed), 16)
    cotangent = gaussian_with(key_list[0], (TOKENS, D), 1.0, 6.0, ((0, 8),), (0, 1, 8, 2.0))
    normed = gaussian(key_list[1], (TOKENS, D), 1.0, 6.0, ((0, 8),))
    inverse_root_mean_square = jnp.clip(jnp.exp(math.log(2.0) - 1.3862944 * jax.random.uniform(key_list[2], (TOKENS,), jnp.float32) ** shard_levels(key_list[2], (TOKENS,), ((0, 8),), -0.2, 0.2)), 0.5, 2.0)
    expert_norm_scale = jnp.clip(1.0 + 0.18 * jax.random.normal(key_list[3], (D,), jnp.float32), 0.1, 1.9)
    routes_keys = jax.random.split(jax.random.fold_in(key_list[4], 1), TOKENS // TOK_DEV)
    routes_turns = jax.random.permutation(jax.random.fold_in(key_list[4], 3), TOKENS // TOK_DEV)
    routes = jax.vmap(lambda own, number: routed_block(jax.random.fold_in(key_list[4], 2), own, number, TOK_DEV, EXPERTS, TOPK, CAP, 1))(routes_keys, routes_turns).reshape((TOKENS, TOPK))
    route_probability_weight = jnp.clip(0.2 + 0.8 * jax.random.uniform(key_list[5], (TOKENS, TOPK), jnp.float32) ** shard_levels(key_list[5], (TOKENS, TOPK), ((0, 8),), -0.2, 0.2), 0.2, 1.0)
    gate_weight = gaussian(key_list[6], (EXPERTS, D, FF), D ** -0.5, 0.125, ((0, 8), (2, 4)))
    up_weight = gaussian(key_list[7], (EXPERTS, D, FF), D ** -0.5, 0.125, ((0, 8), (2, 4)))
    down_weight = gaussian(key_list[8], (EXPERTS, FF, D), FF ** -0.5, 0.125, ((0, 8), (1, 4)))
    recurrence_input = gaussian(key_list[9], (TOKENS, C), 1.0, 6.0, ((0, 8), (1, 4)))
    recurrence_gate_logits = draw_recurrence_gate_logits(jax.random.fold_in(key_list[15], 71), 0)
    input_gate_logits = gaussian(key_list[11], (TOKENS, C), 1.0, 6.0, ((0, 8), (1, 4)))
    channel_decay_weight = draw_channel_decay_weight(jax.random.fold_in(key_list[15], 71), 0)
    extra_log_decay = draw_extra_log_decay(jax.random.fold_in(key_list[15], 71), 0)
    output_matrix = gaussian(key_list[14], (D, C), C ** -0.5, 0.1875, ((1, 4),))
    return dict(cotangent=cotangent, normed=normed, inverse_root_mean_square=inverse_root_mean_square, expert_norm_scale=expert_norm_scale, routes=routes, route_probability_weight=route_probability_weight, gate_weight=gate_weight, up_weight=up_weight, down_weight=down_weight, recurrence_input=recurrence_input, recurrence_gate_logits=recurrence_gate_logits, input_gate_logits=input_gate_logits, channel_decay_weight=channel_decay_weight, extra_log_decay=extra_log_decay, output_matrix=output_matrix)


def link(earlier, later):
    return (earlier[0] * later[0], later[0] * earlier[1] + later[1])

def expert_step(items):
    grad_in, tokens_in, gate_w, up_w, down_w = items
    rows = tokens_in.shape[0]
    gate_pre = jnp.dot(tokens_in, gate_w, preferred_element_type=jnp.float32)
    up_pre = jnp.dot(tokens_in, up_w, preferred_element_type=jnp.float32)
    sigma = jax.nn.sigmoid(gate_pre)
    swish = gate_pre * sigma
    active = (swish * up_pre).astype(jnp.bfloat16)
    d_active = jnp.dot(grad_in, down_w.T, preferred_element_type=jnp.float32)
    d_gate = (d_active * up_pre * sigma * (1.0 + gate_pre * (1.0 - sigma))).astype(jnp.bfloat16)
    d_up = (d_active * swish).astype(jnp.bfloat16)
    grad_down = jnp.dot(active.T, grad_in, preferred_element_type=jnp.float32).astype(jnp.bfloat16)
    grad_gate = jnp.dot(tokens_in.T, d_gate, preferred_element_type=jnp.float32).astype(jnp.bfloat16)
    grad_up = jnp.dot(tokens_in.T, d_up, preferred_element_type=jnp.float32).astype(jnp.bfloat16)
    block = FF // N_TP
    d_gate4 = d_gate.astype(jnp.float32).reshape(rows, N_TP, block)
    d_up4 = d_up.astype(jnp.float32).reshape(rows, N_TP, block)
    gate4 = gate_w.astype(jnp.float32).reshape(D, N_TP, block)
    up4 = up_w.astype(jnp.float32).reshape(D, N_TP, block)
    pieces = jnp.einsum('rjf,djf->jrd', d_gate4, gate4) + jnp.einsum('rjf,djf->jrd', d_up4, up4)
    rounded = lax.optimization_barrier(pieces.astype(jnp.bfloat16)).astype(jnp.float32)
    returned = lax.optimization_barrier(jnp.sum(rounded, axis=0)).astype(jnp.bfloat16)
    return (grad_gate, grad_up, grad_down, returned)

def reference(cotangent, normed, inverse_root_mean_square, expert_norm_scale, routes, route_probability_weight, gate_weight, up_weight, down_weight, recurrence_input, recurrence_gate_logits, input_gate_logits, channel_decay_weight, extra_log_decay, output_matrix):
    per_block = TOK_DEV * TOPK
    chosen = routes.reshape(N_SP, per_block)
    member = (chosen[:, :, None] == jnp.arange(EXPERTS, dtype=jnp.int32)[None, None, :]).astype(jnp.int32)
    ranking = lax.optimization_barrier(jnp.sum((jnp.cumsum(member, axis=1) - member) * member, axis=2))
    source = jnp.arange(N_SP, dtype=jnp.int32)[:, None]
    landing = (chosen * (N_SP * CAP) + source * CAP + ranking).reshape(-1).astype(jnp.int32)
    scaled = (route_probability_weight[:, :, None] * cotangent[:, None, :].astype(jnp.float32)).astype(jnp.bfloat16)
    scaled = scaled.reshape(TOKENS * TOPK, D)
    copies = jnp.repeat(normed, TOPK, axis=0)
    buffer_rows = EXPERTS * N_SP * CAP
    grad_in = jnp.zeros((buffer_rows, D), jnp.bfloat16).at[landing].set(scaled).reshape(EXPERTS, N_SP * CAP, D)
    tokens_in = jnp.zeros((buffer_rows, D), jnp.bfloat16).at[landing].set(copies).reshape(EXPERTS, N_SP * CAP, D)
    grad_gate, grad_up, grad_down, returned = lax.map(expert_step, (grad_in, tokens_in, gate_weight, up_weight, down_weight))
    back_rows = returned.reshape(buffer_rows, D)[landing]
    d_norm = lax.optimization_barrier(jnp.sum(back_rows.astype(jnp.float32).reshape(TOKENS, TOPK, D), axis=1))
    nhat = normed.astype(jnp.float32) / expert_norm_scale[None, :]
    gained = expert_norm_scale[None, :] * d_norm
    stat = lax.optimization_barrier(jnp.mean(gained * nhat, axis=1, keepdims=True))
    d_mix = (cotangent.astype(jnp.float32) + inverse_root_mean_square[:, None] * (gained - nhat * stat)).astype(jnp.bfloat16)
    retention_factor = jax.nn.sigmoid(recurrence_gate_logits.astype(jnp.float32))
    admit = jax.nn.sigmoid(input_gate_logits.astype(jnp.float32))
    signal = recurrence_input.astype(jnp.float32)
    decay_speed = jax.nn.softplus(-channel_decay_weight)
    log_retention = -8.0 * retention_factor * decay_speed[None, :] + extra_log_decay
    keep = jnp.exp(log_retention)
    scale_in = jnp.sqrt(-jnp.expm1(2.0 * log_retention))
    driven = scale_in * admit * signal
    _, state = lax.associative_scan(link, (keep, driven), axis=0)
    hidden = state.astype(jnp.bfloat16)
    state_prev = jnp.concatenate([jnp.zeros((1, C), jnp.float32), state[:-1]], axis=0)
    grad_out_weight = jnp.dot(d_mix.T, hidden, preferred_element_type=jnp.float32)
    d_state = jnp.dot(d_mix, output_matrix, preferred_element_type=jnp.float32)
    keep_next = jnp.concatenate([keep[1:], jnp.ones((1, C), jnp.float32)], axis=0)
    _, total = lax.associative_scan(link, (keep_next, d_state), reverse=True, axis=0)
    grad_rec_input = total * scale_in * admit
    grad_input_gate = total * scale_in * signal * admit * (1.0 - admit)
    d_log = total * state_prev * keep - total * admit * signal * keep * keep / scale_in
    grad_decay_gate = d_log * (-8.0 * decay_speed[None, :]) * retention_factor * (1.0 - retention_factor)
    return (grad_gate, grad_up, grad_down, grad_out_weight, grad_rec_input, grad_decay_gate, grad_input_gate)
```

```python
import functools

import jax
import jax.numpy as jnp
from jax import lax
from jax.experimental import pallas as pl
from jax.experimental.pallas import tpu as pltpu
from jax.sharding import PartitionSpec as P

MESH = pl.DeviceIdType.MESH
VMEM_LIMIT = 63 * 1024 * 1024
F32, BF16 = jnp.float32, jnp.bfloat16
ROWDIMS = (((0,), (0,)), ((), ()))
COLDIMS = (((1,), (1,)), ((), ()))


def sides(m):
    high = max(d for d in range(1, m + 1) if m % d == 0 and d * d <= m)
    return high, m // high


def greet(n, m, me, j):
    barrier = pltpu.get_barrier_semaphore()
    for k in range(1, n):
        pl.semaphore_signal(
            barrier, inc=1, device_id={"sp": lax.rem(me + k, n)}, device_id_type=MESH
        )
    for p in range(1, m):
        pl.semaphore_signal(
            barrier, inc=1, device_id={"tp": lax.rem(j + p, m)}, device_id_type=MESH
        )
    pl.semaphore_wait(barrier, n - 1 + m - 1)


def send(src, dst, send_sem, recv_sem, where):
    return pltpu.make_async_remote_copy(
        src_ref=src,
        dst_ref=dst,
        send_sem=send_sem,
        recv_sem=recv_sem,
        device_id=where,
        device_id_type=MESH,
    )


def scan_rows(a, b, reverse):
    rows = a.shape[0]
    place = lax.broadcasted_iota(jnp.int32, a.shape, 0)
    step = 1
    while step < rows:
        if reverse:
            known = place < rows - step
            shift = rows - step
        else:
            known = place >= step
            shift = step
        a_far = jnp.where(known, pltpu.roll(a, shift, 0), 1.0)
        b_far = jnp.where(known, pltpu.roll(b, shift, 0), 0.0)
        b = a * b_far + b
        a = a * a_far
        step *= 2
    return a, b


def softplus_of_negative(w):
    t = jnp.exp(-jnp.abs(w))
    series = jnp.zeros_like(t)
    for k in range(10, 0, -1):
        series = t * ((1.0 / k if k % 2 else -1.0 / k) + series)
    return jnp.maximum(-w, 0.0) + jnp.where(t < 0.1, series, jnp.log(1.0 + t))


def one_minus_exp(y):
    series = jnp.ones_like(y)
    for k in range(10, 1, -1):
        series = 1.0 + y * (1.0 / k) * series
    return jnp.where(y > -0.5, -y * series, 1.0 - jnp.exp(y))


def block_kernel(
    n, m,
    nrm, cot, routes, probs, irms, gain, rin, rgate, igate, decay, extra, omat, gw, uw, dw,
    ggate, gup, gdown, gow, g_rec, g_dec, g_in,
    xo, co, rtv, pbv, irv, gnv, riv, rgv, igv, dcv, exv, omv, gwv, uwv, dwv,
    info, pos, wgt, keep, scin, admit, retain, cum, loc, prev, hid, carry, enters,
    xg, yg, act, dg, du, pr, stage, red, back, out, hid_all, mix_t, got,
    ld, zs, zr, xs, f1r, f2r, ds, dr, ns, nr, cs, cr, hs, hr, rs, rr, bs, br,
    gs, gr, ms, mr, es, er,
):
    me, j = lax.axis_index("sp"), lax.axis_index("tp")
    tok, feats = nrm.shape
    slots = pr.shape[0]
    cap, q = slots // n, feats // m
    chan, ff = keep.shape[1], gwv.shape[1]
    zn = n // 2
    z, par = lax.div(me, 2), lax.rem(me, 2)
    partner = me + 1 - 2 * par
    high, low = sides(m)
    upper, lower = lax.div(j, low), lax.rem(j, low)
    toks = lambda s: pl.ds(pl.multiple_of(s * tok, tok), tok)
    rows = lambda s: pl.ds(pl.multiple_of(s * cap, cap), cap)
    rows2 = lambda s: pl.ds(pl.multiple_of(s * 2 * cap, 2 * cap), 2 * cap)
    cols = lambda t: pl.ds(pl.multiple_of(t * q, q), q)
    arrays = ((0, xo), (1, co))

    def size(i):
        return low if i == 0 else high

    def near(i, along, across):
        up, down = (across, along) if i == 0 else (along, across)
        return lax.rem(upper + up, high) * low + lax.rem(lower + down, low)

    def source(k):
        fewer = jnp.minimum(z, zn - 1 - z)
        paired = k <= 2 * fewer
        d = jnp.where(paired, lax.div(k + 1, 2), k - fewer)
        odd = lax.rem(k, 2)
        down = jnp.where(paired, odd, jnp.where(z > zn - 1 - z, 1, 0))
        return z + d - 2 * d * down

    loads = [
        pltpu.make_async_copy(src, dst, ld.at[at])
        for at, (src, dst) in enumerate(
            (
                (nrm, xo.at[toks(me)]),
                (cot, co.at[toks(me)]),
                (routes, rtv),
                (probs, pbv),
                (rgate, rgv),
                (decay, dcv),
                (extra, exv),
                (igate, igv),
                (rin, riv),
                (gw.at[0], gwv),
                (uw.at[0], uwv),
                (dw.at[0], dwv),
                (omat, omv),
                (gain, gnv),
                (irms, irv),
            )
        )
    ]
    for c in loads:
        c.start()
    greet(n, m, me, j)
    loads[0].wait()
    loads[1].wait()

    def line(i, o, s, up):
        block = o.at[toks(2 * s + par), cols(j)]
        to = me + 2 if up else me - 2
        return send(block, block, zs.at[i, int(up), s], zr.at[i, s], {"sp": to})

    for i, o in arrays:
        @pl.when(z + 1 < zn)
        def _():
            line(i, o, z, True).start()

        @pl.when(z > 0)
        def _():
            line(i, o, z, False).start()

    def across(i, o, s):
        block = o.at[toks(2 * s + par)]
        return send(block, block, ds.at[i], dr.at[i, s], {"sp": partner})

    for i, o in arrays:
        across(i, o, z).start()

    loads[2].wait()
    loads[3].wait()
    info[me] = jnp.concatenate(
        [rtv[...].astype(F32), pbv[...], jnp.zeros((4, tok), F32)], axis=0
    )

    def told(k):
        to = lax.rem(me + k, n)
        return send(info.at[me], info.at[me], ns, nr.at[k], {"sp": to})

    def tell(k, _):
        told(k).start()
        return 0

    lax.fori_loop(1, n, tell, 0)

    for at in range(4, 9):
        loads[at].wait()
    speed = softplus_of_negative(dcv[...])
    retain[...] = jax.nn.sigmoid(rgv[...].astype(F32))
    admit[...] = jax.nn.sigmoid(igv[...].astype(F32))
    log_keep = -8.0 * retain[...] * speed + exv[...]
    keep[...] = jnp.exp(log_keep)
    scin[...] = jnp.sqrt(one_minus_exp(2.0 * log_keep))
    a, b = scan_rows(keep[...], scin[...] * admit[...] * riv[...].astype(F32), False)
    cum[...] = a
    loc[...] = b
    carry[me] = jnp.concatenate(
        [a[tok - 1 : tok], b[tok - 1 : tok], jnp.zeros((6, chan), F32)], axis=0
    )

    def carried(k):
        to = lax.rem(me + k, n)
        return send(carry.at[me], carry.at[me], cs, cr.at[k], {"sp": to})

    def start_carry(k, _):
        carried(k).start()
        return 0

    lax.fori_loop(1, n, start_carry, 0)

    earlier = (
        lax.broadcasted_iota(jnp.int32, (tok, tok), 0)
        < lax.broadcasted_iota(jnp.int32, (tok, tok), 1)
    ).astype(F32).astype(BF16)

    def place(k, _):
        s = lax.rem(me - k + n, n)

        @pl.when(k > 0)
        def _():
            send(info.at[s], info.at[s], ns, nr.at[k], {"sp": s}).wait_recv()

        mine = info[s]
        first, second = mine[0:1] == me.astype(F32), mine[1:2] == me.astype(F32)
        member = jnp.where(jnp.logical_or(first, second), 1.0, 0.0)
        wide = jnp.broadcast_to(member, (8, tok))
        ranking = jnp.dot(wide.astype(BF16), earlier, preferred_element_type=F32)
        pos[s] = jnp.where(wide > 0.0, ranking, -1.0)
        weight = jnp.where(first, mine[2:3], 0.0) + jnp.where(second, mine[3:4], 0.0)
        wgt[s] = jnp.broadcast_to(weight, (8, tok))
        return 0

    lax.fori_loop(0, n, place, 0)
    for at in range(9, 15):
        loads[at].wait()

    def onward(s, i, o):
        block = o.at[toks(2 * s + par), cols(j)]
        for p in range(1, size(i)):
            send(block, block, xs.at[i], f1r.at[i, s], {"tp": near(i, p, 0)}).start()
        for p in range(1, size(1 - i)):
            send(block, block, xs.at[i], f2r.at[i, s], {"tp": near(i, 0, p)}).start()

    def several(o, s, count):
        return o.at[toks(2 * s + par), pl.ds(0, count * q)]

    def relayed(s):
        for i, o in arrays:
            if size(i) > 1:
                part = several(o, s, size(i) - 1)
                send(part, part, xs.at[i], f1r.at[i, s], {"tp": near(i, 1, 0)}).wait_recv()
            for c in range(1, size(i)):
                block = o.at[toks(2 * s + par), cols(near(i, size(i) - c, 0))]
                for p in range(1, size(1 - i)):
                    send(block, block, xs.at[i], f2r.at[i, s], {"tp": near(i, 0, p)}).start()

    def whole(s):
        for i, o in arrays:
            if size(1 - i) > 1:
                part = several(o, s, m - size(i))
                send(part, part, xs.at[i], f2r.at[i, s], {"tp": near(i, 0, 1)}).wait_recv()
            across(i, o, s).start()

    span = min(feats, 512)
    unit = min(ff, 256)

    def compute(s):
        other = 2 * s + 1 - par
        for i, o in arrays:
            block = o.at[toks(other)]
            send(block, block, ds.at[i], dr.at[i, s], {"sp": partner}).wait_recv()
        low_at, high_at = pos[2 * s][0:1], pos[2 * s + 1][0:1]
        high_at = jnp.where(high_at >= 0.0, high_at + float(cap), -1.0)
        at = jnp.concatenate([low_at, high_at], axis=1)
        weight = jnp.concatenate([wgt[2 * s][0:1], wgt[2 * s + 1][0:1]], axis=1)
        here = lax.broadcasted_iota(jnp.int32, (2 * cap, 2 * tok), 0).astype(F32)
        hit = here == at
        one = jnp.where(hit, 1.0, 0.0)
        share = jnp.sum(jnp.where(hit, weight, 0.0), axis=1, keepdims=True)
        one = one.astype(BF16)
        pair = pl.ds(pl.multiple_of(s * 2 * tok, 2 * tok), 2 * tok)
        land = rows2(s)
        for t in range(feats // span):
            f = pl.ds(t * span, span)
            xg[land, f] = jnp.dot(one, xo[pair, f], preferred_element_type=F32).astype(BF16)
            yg[land, f] = (share * jnp.dot(one, co[pair, f], preferred_element_type=F32)).astype(
                BF16
            )
        for t in range(ff // unit):
            f = pl.ds(t * unit, unit)
            gate = jnp.dot(xg[land, :], gwv[:, f], preferred_element_type=F32)
            up = jnp.dot(xg[land, :], uwv[:, f], preferred_element_type=F32)
            d_act = lax.dot_general(yg[land, :], dwv[f, :], COLDIMS, preferred_element_type=F32)
            sigma = jax.nn.sigmoid(gate)
            swish = gate * sigma
            act[land, f] = (swish * up).astype(BF16)
            dg[land, f] = (d_act * up * sigma * (1.0 + gate * (1.0 - sigma))).astype(BF16)
            du[land, f] = (d_act * swish).astype(BF16)
        for t in range(feats // span):
            f = pl.ds(t * span, span)
            part = lax.dot_general(dg[land, :], gwv[f, :], COLDIMS, preferred_element_type=F32)
            part += lax.dot_general(du[land, :], uwv[f, :], COLDIMS, preferred_element_type=F32)
            pr[land, f] = part.astype(BF16)
        for p in range(1, m):
            far = lax.rem(j + p, m)
            send(
                pr.at[land, cols(far)], stage.at[p - 1, land], rs.at[s], rr.at[s], {"tp": far}
            ).start()

    def shipped(s):
        return send(red.at[rows(s)], back.at[rows(me)], bs, br.at[me], {"sp": s})

    def reduce(s):
        land = rows2(s)
        block = stage.at[:, land]
        arrived = send(block, block, rs.at[s], rr.at[s], {"tp": lax.rem(j + 1, m)})
        arrived.wait_recv()
        arrived.wait_send()
        total = pr[land, cols(j)].astype(F32)
        for p in range(1, m):
            total = total + stage[p - 1, land].astype(F32)
        red[land] = total.astype(BF16)
        for c in range(2):
            @pl.when(2 * s + c != me)
            def _():
                shipped(2 * s + c).start()

    def step(k, _):
        @pl.when(k < zn)
        def _():
            s = source(k)
            for i, o in arrays:
                line(i, o, s, True).wait_recv()

                @pl.when(jnp.logical_and(s < z, z + 1 < zn))
                def _():
                    line(i, o, s, True).start()

                @pl.when(jnp.logical_and(s > z, z > 0))
                def _():
                    line(i, o, s, False).start()

                onward(s, i, o)

        @pl.when(jnp.logical_and(k >= 2, k < zn + 1))
        def _():
            relayed(source(k - 1))

        @pl.when(k >= 3)
        def _():
            whole(source(k - 2))

        @pl.when(jnp.logical_or(k == 1, k >= 3))
        def _():
            compute(source(jnp.where(k == 1, 0, k - 2)))

        @pl.when(k >= 3)
        def _():
            reduce(source(k - 3))

        return 0

    lax.fori_loop(1, zn + 2, step, 0)

    def take_carry(k, _):
        s = lax.rem(me - k + n, n)
        send(carry.at[s], carry.at[s], cs, cr.at[k], {"sp": s}).wait_recv()
        return 0

    lax.fori_loop(1, n, take_carry, 0)
    state = jnp.zeros((1, chan), F32)
    for s in range(n):
        state = jnp.where(s < me, carry[s, 0:1] * state + carry[s, 1:2], state)
    states = loc[...] + cum[...] * state
    hid[...] = states.astype(BF16)
    spot = lax.broadcasted_iota(jnp.int32, (tok, chan), 0)
    prev[...] = jnp.where(spot >= 1, pltpu.roll(states, 1, 0), state)
    hid_all[me] = hid[...]

    def shared(k):
        to = lax.rem(me + k, n)
        return send(hid, hid_all.at[me], hs, hr.at[k], {"sp": to})

    def share_hidden(k, _):
        shared(k).start()
        return 0

    lax.fori_loop(1, n, share_hidden, 0)

    def wide_grads(t, _):
        f = pl.ds(pl.multiple_of(t * 256, 256), 256)
        rowsof = xg[:, f]
        ggate[0, f, :] = lax.dot_general(
            rowsof, dg[...], ROWDIMS, preferred_element_type=F32
        ).astype(BF16)
        gup[0, f, :] = lax.dot_general(
            rowsof, du[...], ROWDIMS, preferred_element_type=F32
        ).astype(BF16)
        return 0

    lax.fori_loop(0, feats // 256, wide_grads, 0)
    for t in range(ff // min(ff, 128)):
        f = pl.ds(t * min(ff, 128), min(ff, 128))
        gdown[0, f, :] = lax.dot_general(
            act[:, f], yg[...], ROWDIMS, preferred_element_type=F32
        ).astype(BF16)

    reduce(source(zn - 1))
    back[rows(me)] = red[rows(me)]

    own = info[me]
    experts = lax.broadcasted_iota(jnp.int32, (n, tok), 0).astype(F32)
    member = jnp.where(jnp.logical_or(own[0:1] == experts, own[1:2] == experts), 1.0, 0.0)
    ranking = jnp.dot(member.astype(BF16), earlier, preferred_element_type=F32)
    ranking = jnp.where(member > 0.0, ranking, -1.0)
    depth = lax.broadcasted_iota(jnp.int32, (n, cap, tok), 1).astype(F32)
    pick = jnp.where(depth == ranking[:, None, :], 1.0, 0.0).reshape(slots, tok).astype(BF16)

    def collect(k, _):
        s = lax.rem(me - k + n, n)
        block = back.at[rows(s)]
        send(block, block, bs, br.at[s], {"sp": s}).wait_recv()
        return 0

    lax.fori_loop(1, n, collect, 0)
    total = lax.dot_general(pick, back[...], ROWDIMS, preferred_element_type=F32)
    out[:, cols(j)] = total.astype(BF16)
    mine = out.at[:, cols(j)]
    for p in range(1, m):
        send(mine, mine, gs.at[p], gr.at[p], {"tp": lax.rem(j + p, m)}).start()
    for p in range(1, m):
        far = lax.rem(j - p + m, m)
        theirs = out.at[:, cols(far)]
        send(mine, mine, gs.at[p], gr.at[p], {"tp": far}).wait_send()
        send(theirs, theirs, gs.at[p], gr.at[p], {"tp": far}).wait_recv()

    slab = feats // n
    slabs = lambda s: pl.ds(pl.multiple_of(s * slab, slab), slab)
    scale = gnv[...]
    nhat = xo[toks(me)].astype(F32) / scale
    gained = scale * out[...].astype(F32)
    stat = jnp.mean(gained * nhat, axis=1, keepdims=True)
    root = jnp.broadcast_to(irv[...], (8, tok)).T[:, 0:1]
    mixed = co[toks(me)].astype(F32) + root * (gained - nhat * stat)
    mix_t[...] = mixed.T.astype(BF16)

    def blocks(k):
        to = lax.rem(me + k, n)
        return send(mix_t.at[slabs(to)], got.at[me], ms, mr.at[k], {"sp": to})

    def start_blocks(k, _):
        blocks(k).start()
        return 0

    lax.fori_loop(1, n, start_blocks, 0)
    d_state = jnp.dot(mixed.astype(BF16), omv[...], preferred_element_type=F32)
    here = keep[...]
    after = jnp.where(spot < tok - 1, pltpu.roll(here, tok - 1, 0), 1.0)
    a, b = scan_rows(after, d_state, True)
    enters[me] = jnp.broadcast_to(here[0:1] * b[0:1], (8, chan))
    cum[...] = a
    loc[...] = b

    def entering(k):
        to = lax.rem(me + k, n)
        return send(enters.at[me], enters.at[me], es, er.at[k], {"sp": to})

    def start_enter(k, _):
        entering(k).start()
        return 0

    lax.fori_loop(1, n, start_enter, 0)
    gow[...] = jnp.dot(mix_t[slabs(me)], hid_all[me], preferred_element_type=F32)

    def take_hidden(k, _):
        s = lax.rem(me - k + n, n)
        send(hid, hid_all.at[s], hs, hr.at[k], {"sp": s}).wait_recv()
        return 0

    lax.fori_loop(1, n, take_hidden, 0)

    def add(k, _):
        s = lax.rem(me - k + n, n)
        send(got.at[s], got.at[s], ms, mr.at[k], {"sp": s}).wait_recv()
        gow[...] += jnp.dot(got[s], hid_all[s], preferred_element_type=F32)
        return 0

    lax.fori_loop(1, n, add, 0)

    def take_enter(k, _):
        s = lax.rem(me - k + n, n)
        send(enters.at[s], enters.at[s], es, er.at[k], {"sp": s}).wait_recv()
        return 0

    lax.fori_loop(1, n, take_enter, 0)
    enter = jnp.zeros((1, chan), F32)
    for s in range(n - 1, -1, -1):
        enter = jnp.where(s > me, carry[s, 0:1] * enter + enters[s, 0:1], enter)
    total = loc[...] + cum[...] * enter
    inward, opened, held, kept = scin[...], admit[...], retain[...], keep[...]
    signal = riv[...].astype(F32)
    g_rec[...] = total * inward * opened
    g_in[...] = total * inward * signal * opened * (1.0 - opened)
    d_log = total * prev[...] * kept - total * opened * signal * kept * kept / inward
    g_dec[...] = d_log * (-8.0 * speed) * held * (1.0 - held)

    def flush(s, _):
        for i, o in arrays:
            @pl.when(jnp.logical_and(s <= z, z + 1 < zn))
            def _():
                line(i, o, s, True).wait_send()

            @pl.when(jnp.logical_and(s >= z, z > 0))
            def _():
                line(i, o, s, False).wait_send()

        return 0

    lax.fori_loop(0, zn, flush, 0)
    for i, o in arrays:
        part = o.at[pl.ds(0, (zn - 1) * tok), pl.ds(0, (m - 1) * q)]
        send(part, part, xs.at[i], f1r.at[i, 0], {"tp": lax.rem(j + 1, m)}).wait_send()
        part = o.at[pl.ds(0, zn * tok)]
        send(part, part, ds.at[i], dr.at[i, 0], {"sp": partner}).wait_send()
    to = {"sp": partner}
    others = pl.ds(0, n - 1)
    send(info.at[others], info.at[others], ns, nr.at[0], to).wait_send()
    send(carry.at[others], carry.at[others], cs, cr.at[0], to).wait_send()
    send(enters.at[others], enters.at[others], es, er.at[0], to).wait_send()
    send(hid_all.at[others], hid_all.at[others], hs, hr.at[0], to).wait_send()
    send(got.at[others], got.at[others], ms, mr.at[0], to).wait_send()
    part = red.at[pl.ds(0, (n - 1) * cap)]
    send(part, part, bs, br.at[0], to).wait_send()


def shards(
    cotangent,
    normed,
    inverse_root_mean_square,
    expert_norm_scale,
    routes,
    route_probability_weight,
    gate_weight,
    up_weight,
    down_weight,
    recurrence_input,
    recurrence_gate_logits,
    input_gate_logits,
    channel_decay_weight,
    extra_log_decay,
    output_matrix,
):
    tok, feats = normed.shape
    n, m = lax.axis_size("sp"), lax.axis_size("tp")
    picks = routes.shape[1]
    cap = 2 * picks * tok // n
    slots = n * cap
    q = feats // m
    ff = gate_weight.shape[2]
    chan = recurrence_input.shape[1]
    zn = n // 2
    dma = pltpu.SemaphoreType.DMA
    vmem = lambda *s: pltpu.VMEM(s, F32)
    half = lambda *s: pltpu.VMEM(s, BF16)
    outs = [
        ((1, feats, ff), BF16),
        ((1, feats, ff), BF16),
        ((1, ff, feats), BF16),
        ((feats // n, chan), F32),
        ((tok, chan), F32),
        ((tok, chan), F32),
        ((tok, chan), F32),
    ]
    scratch = [
        half(n * tok, feats),
        half(n * tok, feats),
        pltpu.VMEM((picks, tok), jnp.int32),
        vmem(picks, tok),
        vmem(1, tok),
        vmem(1, feats),
        half(tok, chan),
        half(tok, chan),
        half(tok, chan),
        vmem(1, chan),
        vmem(tok, chan),
        half(feats, chan),
        half(feats, ff),
        half(feats, ff),
        half(ff, feats),
        vmem(n, 8, tok),
        vmem(n, 8, tok),
        vmem(n, 8, tok),
        vmem(tok, chan),
        vmem(tok, chan),
        vmem(tok, chan),
        vmem(tok, chan),
        vmem(tok, chan),
        vmem(tok, chan),
        vmem(tok, chan),
        half(tok, chan),
        vmem(n, 8, chan),
        vmem(n, 8, chan),
        half(slots, feats),
        half(slots, feats),
        half(slots, ff),
        half(slots, ff),
        half(slots, ff),
        half(slots, feats),
        half(m - 1, slots, q),
        half(slots, q),
        half(slots, q),
        half(tok, feats),
        half(n, tok, chan),
        half(feats, tok),
        half(n, feats // n, tok),
        dma((15,)),
        dma((2, 2, zn)),
        dma((2, zn)),
        dma((2,)),
        dma((2, zn)),
        dma((2, zn)),
        dma((2,)),
        dma((2, zn)),
        dma,
        dma((n,)),
        dma,
        dma((n,)),
        dma,
        dma((n,)),
        dma((zn,)),
        dma((zn,)),
        dma,
        dma((n,)),
        dma((m,)),
        dma((m,)),
        dma,
        dma((n,)),
        dma,
        dma((n,)),
    ]
    args = (
        normed,
        cotangent,
        routes.T,
        route_probability_weight.T,
        inverse_root_mean_square[None, :],
        expert_norm_scale[None, :],
        recurrence_input,
        recurrence_gate_logits,
        input_gate_logits,
        channel_decay_weight[None, :],
        extra_log_decay,
        output_matrix,
        gate_weight,
        up_weight,
        down_weight,
    )
    return pl.pallas_call(
        functools.partial(block_kernel, n, m),
        out_shape=tuple(jax.ShapeDtypeStruct(s, d) for s, d in outs),
        in_specs=[pl.BlockSpec(memory_space=pl.ANY)] * len(args),
        out_specs=tuple(pl.BlockSpec(memory_space=pltpu.VMEM) for _ in outs),
        scratch_shapes=scratch,
        compiler_params=pltpu.CompilerParams(
            collective_id=0, has_side_effects=True, vmem_limit_bytes=VMEM_LIMIT
        ),
    )(*args)


def solution(mesh):
    return jax.shard_map(
        shards,
        mesh=mesh,
        in_specs=(
            P("sp", None),
            P("sp", None),
            P("sp"),
            P(),
            P("sp", None),
            P("sp", None),
            P("sp", None, "tp"),
            P("sp", None, "tp"),
            P("sp", "tp", None),
            P("sp", "tp"),
            P("sp", "tp"),
            P("sp", "tp"),
            P("tp"),
            P("sp", "tp"),
            P(None, "tp"),
        ),
        out_specs=(
            P("sp", None, "tp"),
            P("sp", None, "tp"),
            P("sp", "tp", None),
            P("sp", "tp"),
            P("sp", "tp"),
            P("sp", "tp"),
            P("sp", "tp"),
        ),
        check_vma=False,
    )
```

```python
import functools

import jax
import jax.numpy as jnp
from jax import lax
from jax.experimental import pallas as pl
from jax.experimental.pallas import tpu as pltpu
from jax.sharding import PartitionSpec as P

MESH = pl.DeviceIdType.MESH
VMEM_LIMIT = 63 * 1024 * 1024
SPARE = 8 * 1024 * 1024
LEAST = 12 * 1024 * 1024
F32, BF16 = jnp.float32, jnp.bfloat16
ROWDIMS = (((0,), (0,)), ((), ()))
COLDIMS = (((1,), (1,)), ((), ()))


def sides(m):
    high = max(d for d in range(1, m + 1) if m % d == 0 and d * d <= m)
    return high, m // high


def greet(n, m, me, j):
    barrier = pltpu.get_barrier_semaphore()
    for k in range(1, n):
        pl.semaphore_signal(
            barrier, inc=1, device_id={"sp": lax.rem(me + k, n)}, device_id_type=MESH
        )
    for p in range(1, m):
        pl.semaphore_signal(
            barrier, inc=1, device_id={"tp": lax.rem(j + p, m)}, device_id_type=MESH
        )
    pl.semaphore_wait(barrier, n - 1 + m - 1)


def send(src, dst, send_sem, recv_sem, where):
    return pltpu.make_async_remote_copy(
        src_ref=src,
        dst_ref=dst,
        send_sem=send_sem,
        recv_sem=recv_sem,
        device_id=where,
        device_id_type=MESH,
    )


def scan_rows(a, b, reverse):
    rows = a.shape[0]
    place = lax.broadcasted_iota(jnp.int32, a.shape, 0)
    step = 1
    while step < rows:
        if reverse:
            known = place < rows - step
            shift = rows - step
        else:
            known = place >= step
            shift = step
        a_far = jnp.where(known, pltpu.roll(a, shift, 0), 1.0)
        b_far = jnp.where(known, pltpu.roll(b, shift, 0), 0.0)
        b = a * b_far + b
        a = a * a_far
        step *= 2
    return a, b


def softplus_of_negative(w):
    t = jnp.exp(-jnp.abs(w))
    series = jnp.zeros_like(t)
    for k in range(10, 0, -1):
        series = t * ((1.0 / k if k % 2 else -1.0 / k) + series)
    return jnp.maximum(-w, 0.0) + jnp.where(t < 0.1, series, jnp.log(1.0 + t))


def one_minus_exp(y):
    series = jnp.ones_like(y)
    for k in range(10, 1, -1):
        series = 1.0 + y * (1.0 / k) * series
    return jnp.where(y > -0.5, -y * series, 1.0 - jnp.exp(y))


def block_kernel(
    n, m,
    nrm, cot, routes, probs, irms, gain, rin, rgate, igate, decay, extra, omat, gw, uw, dw,
    ggate, gup, gdown, gow, g_rec, g_dec, g_in,
    xo, co, rtv, pbv, irv, gnv, riv, rgv, igv, dcv, exv, omv, gwv, uwv, dwv,
    info, keep, scin, admit, retain, cum, loc, prev, hid, carry, enters,
    xg, yg, act, dg, du, pr, stage, red, back, out, hid_all, mix_t, got,
    ld, zs, zr, xs, f1r, f2r, ds, dr, ns, nr, cs, cr, hs, hr, rs, rr, bs, br,
    gs, gr, ms, mr, es, er,
):
    me, j = lax.axis_index("sp"), lax.axis_index("tp")
    tok, feats = nrm.shape
    slots = pr.shape[0]
    cap, q = slots // n, feats // m
    chan, ff = keep.shape[1], gwv.shape[1]
    zn = n // 2
    z, par = lax.div(me, 2), lax.rem(me, 2)
    partner = me + 1 - 2 * par
    high, low = sides(m)
    upper, lower = lax.div(j, low), lax.rem(j, low)
    toks = lambda s: pl.ds(pl.multiple_of(s * tok, tok), tok)
    rows = lambda s: pl.ds(pl.multiple_of(s * cap, cap), cap)
    rows2 = lambda s: pl.ds(pl.multiple_of(s * 2 * cap, 2 * cap), 2 * cap)
    cols = lambda t: pl.ds(pl.multiple_of(t * q, q), q)
    arrays = ((0, xo), (1, co))

    def size(i):
        return low if i == 0 else high

    def near(i, along, across):
        up, down = (across, along) if i == 0 else (along, across)
        return lax.rem(upper + up, high) * low + lax.rem(lower + down, low)

    def source(k):
        fewer = jnp.minimum(z, zn - 1 - z)
        paired = k <= 2 * fewer
        d = jnp.where(paired, lax.div(k + 1, 2), k - fewer)
        odd = lax.rem(k, 2)
        down = jnp.where(paired, odd, jnp.where(z > zn - 1 - z, 1, 0))
        return z + d - 2 * d * down

    loads = [
        pltpu.make_async_copy(src, dst, ld.at[at])
        for at, (src, dst) in enumerate(
            (
                (routes, rtv),
                (probs, pbv),
                (nrm, xo.at[toks(me)]),
                (cot, co.at[toks(me)]),
                (rgate, rgv),
                (decay, dcv),
                (extra, exv),
                (igate, igv),
                (rin, riv),
                (gw.at[0], gwv),
                (uw.at[0], uwv),
                (dw.at[0], dwv),
                (omat, omv),
                (gain, gnv),
                (irms, irv),
            )
        )
    ]
    for c in loads:
        c.start()
    greet(n, m, me, j)
    loads[0].wait()
    loads[1].wait()
    info[me] = jnp.concatenate(
        [rtv[...].astype(F32), pbv[...], jnp.zeros((4, tok), F32)], axis=0
    )

    def told(k):
        to = lax.rem(me + k, n)
        return send(info.at[me], info.at[me], ns, nr.at[me], {"sp": to})

    def tell(k, _):
        told(k).start()
        return 0

    lax.fori_loop(1, n, tell, 0)

    loads[2].wait()
    loads[3].wait()

    def line(i, o, s, up):
        block = o.at[toks(2 * s + par), cols(j)]
        to = me + 2 if up else me - 2
        return send(block, block, zs.at[i, int(up), s], zr.at[i, s], {"sp": to})

    for i, o in arrays:
        @pl.when(z + 1 < zn)
        def _():
            line(i, o, z, True).start()

        @pl.when(z > 0)
        def _():
            line(i, o, z, False).start()

    def across(i, o, s):
        block = o.at[toks(2 * s + par)]
        return send(block, block, ds.at[i], dr.at[i, s], {"sp": partner})

    for i, o in arrays:
        across(i, o, z).start()

    for at in range(4, 9):
        loads[at].wait()
    speed = softplus_of_negative(dcv[...])
    retain[...] = jax.nn.sigmoid(rgv[...].astype(F32))
    admit[...] = jax.nn.sigmoid(igv[...].astype(F32))
    log_keep = -8.0 * retain[...] * speed + exv[...]
    keep[...] = jnp.exp(log_keep)
    scin[...] = jnp.sqrt(one_minus_exp(2.0 * log_keep))
    a, b = scan_rows(keep[...], scin[...] * admit[...] * riv[...].astype(F32), False)
    cum[...] = a
    loc[...] = b
    carry[me] = jnp.concatenate(
        [a[tok - 1 : tok], b[tok - 1 : tok], jnp.zeros((6, chan), F32)], axis=0
    )

    def carried(k):
        to = lax.rem(me + k, n)
        return send(carry.at[me], carry.at[me], cs, cr.at[k], {"sp": to})

    def start_carry(k, _):
        carried(k).start()
        return 0

    lax.fori_loop(1, n, start_carry, 0)

    earlier = (
        lax.broadcasted_iota(jnp.int32, (tok, tok), 0)
        < lax.broadcasted_iota(jnp.int32, (tok, tok), 1)
    ).astype(F32).astype(BF16)

    def place(s):
        @pl.when(s != me)
        def _():
            send(info.at[s], info.at[s], ns, nr.at[s], {"sp": s}).wait_recv()

        mine = info[s]
        first, second = mine[0:1] == me.astype(F32), mine[1:2] == me.astype(F32)
        member = jnp.where(jnp.logical_or(first, second), 1.0, 0.0)
        wide = jnp.broadcast_to(member, (8, tok))
        ranking = jnp.dot(wide.astype(BF16), earlier, preferred_element_type=F32)
        weight = jnp.where(first, mine[2:3], 0.0) + jnp.where(second, mine[3:4], 0.0)
        return jnp.where(member > 0.0, ranking[0:1], -1.0), weight

    for at in range(9, 15):
        loads[at].wait()

    def onward(s, i, o):
        block = o.at[toks(2 * s + par), cols(j)]
        for p in range(1, size(i)):
            send(block, block, xs.at[i], f1r.at[i, s], {"tp": near(i, p, 0)}).start()
        for p in range(1, size(1 - i)):
            send(block, block, xs.at[i], f2r.at[i, s], {"tp": near(i, 0, p)}).start()

    def several(o, s, count):
        return o.at[toks(2 * s + par), pl.ds(0, count * q)]

    def relayed(s):
        for i, o in arrays:
            if size(i) > 1:
                part = several(o, s, size(i) - 1)
                send(part, part, xs.at[i], f1r.at[i, s], {"tp": near(i, 1, 0)}).wait_recv()
            for c in range(1, size(i)):
                block = o.at[toks(2 * s + par), cols(near(i, size(i) - c, 0))]
                for p in range(1, size(1 - i)):
                    send(block, block, xs.at[i], f2r.at[i, s], {"tp": near(i, 0, p)}).start()

    def whole(s):
        for i, o in arrays:
            if size(1 - i) > 1:
                part = several(o, s, m - size(i))
                send(part, part, xs.at[i], f2r.at[i, s], {"tp": near(i, 0, 1)}).wait_recv()
            across(i, o, s).start()

    span = min(feats, 512)
    unit = min(ff, 256)

    def compute(s):
        other = 2 * s + 1 - par
        for i, o in arrays:
            block = o.at[toks(other)]
            send(block, block, ds.at[i], dr.at[i, s], {"sp": partner}).wait_recv()
        (low_at, low_weight), (high_at, high_weight) = place(2 * s), place(2 * s + 1)
        high_at = jnp.where(high_at >= 0.0, high_at + float(cap), -1.0)
        at = jnp.concatenate([low_at, high_at], axis=1)
        weight = jnp.concatenate([low_weight, high_weight], axis=1)
        here = lax.broadcasted_iota(jnp.int32, (2 * cap, 2 * tok), 0).astype(F32)
        hit = here == at
        one = jnp.where(hit, 1.0, 0.0)
        share = jnp.sum(jnp.where(hit, weight, 0.0), axis=1, keepdims=True)
        one = one.astype(BF16)
        pair = pl.ds(pl.multiple_of(s * 2 * tok, 2 * tok), 2 * tok)
        land = rows2(s)
        for t in range(feats // span):
            f = pl.ds(t * span, span)
            xg[land, f] = jnp.dot(one, xo[pair, f], preferred_element_type=F32).astype(BF16)
            yg[land, f] = (share * jnp.dot(one, co[pair, f], preferred_element_type=F32)).astype(
                BF16
            )
        for t in range(ff // unit):
            f = pl.ds(t * unit, unit)
            gate = jnp.dot(xg[land, :], gwv[:, f], preferred_element_type=F32)
            up = jnp.dot(xg[land, :], uwv[:, f], preferred_element_type=F32)
            d_act = lax.dot_general(yg[land, :], dwv[f, :], COLDIMS, preferred_element_type=F32)
            sigma = jax.nn.sigmoid(gate)
            swish = gate * sigma
            act[land, f] = (swish * up).astype(BF16)
            dg[land, f] = (d_act * up * sigma * (1.0 + gate * (1.0 - sigma))).astype(BF16)
            du[land, f] = (d_act * swish).astype(BF16)
        for t in range(feats // span):
            f = pl.ds(t * span, span)
            part = lax.dot_general(dg[land, :], gwv[f, :], COLDIMS, preferred_element_type=F32)
            part += lax.dot_general(du[land, :], uwv[f, :], COLDIMS, preferred_element_type=F32)
            pr[land, f] = part.astype(BF16)
        for p in range(1, m):
            far = lax.rem(j + p, m)
            send(
                pr.at[land, cols(far)], stage.at[p - 1, land], rs.at[s], rr.at[s], {"tp": far}
            ).start()

    def shipped(s):
        return send(red.at[rows(s)], back.at[rows(me)], bs, br.at[me], {"sp": s})

    def reduce(s):
        land = rows2(s)
        block = stage.at[:, land]
        arrived = send(block, block, rs.at[s], rr.at[s], {"tp": lax.rem(j + 1, m)})
        arrived.wait_recv()
        arrived.wait_send()
        total = pr[land, cols(j)].astype(F32)
        for p in range(1, m):
            total = total + stage[p - 1, land].astype(F32)
        red[land] = total.astype(BF16)
        for c in range(2):
            @pl.when(2 * s + c != me)
            def _():
                shipped(2 * s + c).start()

    spot = lax.broadcasted_iota(jnp.int32, (tok, chan), 0)

    def hidden():
        def take_carry(k, _):
            s = lax.rem(me - k + n, n)
            send(carry.at[s], carry.at[s], cs, cr.at[k], {"sp": s}).wait_recv()
            return 0

        lax.fori_loop(1, n, take_carry, 0)
        state = jnp.zeros((1, chan), F32)
        for s in range(n):
            state = jnp.where(s < me, carry[s, 0:1] * state + carry[s, 1:2], state)
        states = loc[...] + cum[...] * state
        hid[...] = states.astype(BF16)
        prev[...] = jnp.where(spot >= 1, pltpu.roll(states, 1, 0), state)
        hid_all[me] = hid[...]

        def shared(k):
            to = lax.rem(me + k, n)
            return send(hid, hid_all.at[me], hs, hr.at[k], {"sp": to})

        def share_hidden(k, _):
            shared(k).start()
            return 0

        lax.fori_loop(1, n, share_hidden, 0)

    def step(k, _):
        @pl.when(jnp.logical_and(k >= 1, k < zn))
        def _():
            s = source(k)
            for i, o in arrays:
                line(i, o, s, True).wait_recv()

                @pl.when(jnp.logical_and(s < z, z + 1 < zn))
                def _():
                    line(i, o, s, True).start()

                @pl.when(jnp.logical_and(s > z, z > 0))
                def _():
                    line(i, o, s, False).start()

                onward(s, i, o)

        @pl.when(k == zn - 1)
        def _():
            hidden()

        @pl.when(jnp.logical_and(k >= 2, k < zn + 1))
        def _():
            relayed(source(k - 1))

        @pl.when(k >= 3)
        def _():
            whole(source(k - 2))

        @pl.when(jnp.logical_or(k == 0, k >= 3))
        def _():
            compute(source(jnp.where(k == 0, 0, k - 2)))

        @pl.when(k >= 3)
        def _():
            reduce(source(k - 3))

        return 0

    lax.fori_loop(0, zn + 2, step, 0)

    def wide_grads(t, _):
        f = pl.ds(pl.multiple_of(t * 256, 256), 256)
        rowsof = xg[:, f]
        ggate[0, f, :] = lax.dot_general(
            rowsof, dg[...], ROWDIMS, preferred_element_type=F32
        ).astype(BF16)
        gup[0, f, :] = lax.dot_general(
            rowsof, du[...], ROWDIMS, preferred_element_type=F32
        ).astype(BF16)
        return 0

    lax.fori_loop(0, feats // 256, wide_grads, 0)
    for t in range(ff // min(ff, 128)):
        f = pl.ds(t * min(ff, 128), min(ff, 128))
        gdown[0, f, :] = lax.dot_general(
            act[:, f], yg[...], ROWDIMS, preferred_element_type=F32
        ).astype(BF16)

    reduce(source(zn - 1))
    back[rows(me)] = red[rows(me)]

    own = info[me]
    experts = lax.broadcasted_iota(jnp.int32, (n, tok), 0).astype(F32)
    member = jnp.where(jnp.logical_or(own[0:1] == experts, own[1:2] == experts), 1.0, 0.0)
    ranking = jnp.dot(member.astype(BF16), earlier, preferred_element_type=F32)
    ranking = jnp.where(member > 0.0, ranking, -1.0)
    depth = lax.broadcasted_iota(jnp.int32, (n, cap, tok), 1).astype(F32)
    pick = jnp.where(depth == ranking[:, None, :], 1.0, 0.0).reshape(slots, tok).astype(BF16)

    def collect(k, _):
        s = lax.rem(me - k + n, n)
        block = back.at[rows(s)]
        send(block, block, bs, br.at[s], {"sp": s}).wait_recv()
        return 0

    lax.fori_loop(1, n, collect, 0)
    total = lax.dot_general(pick, back[...], ROWDIMS, preferred_element_type=F32)
    out[:, cols(j)] = total.astype(BF16)
    mine = out.at[:, cols(j)]
    for p in range(1, m):
        send(mine, mine, gs.at[p], gr.at[p], {"tp": lax.rem(j + p, m)}).start()
    for p in range(1, m):
        far = lax.rem(j - p + m, m)
        theirs = out.at[:, cols(far)]
        send(mine, mine, gs.at[p], gr.at[p], {"tp": far}).wait_send()
        send(theirs, theirs, gs.at[p], gr.at[p], {"tp": far}).wait_recv()

    slab = feats // n
    slabs = lambda s: pl.ds(pl.multiple_of(s * slab, slab), slab)
    scale = gnv[...]
    nhat = xo[toks(me)].astype(F32) / scale
    gained = scale * out[...].astype(F32)
    stat = jnp.mean(gained * nhat, axis=1, keepdims=True)
    root = jnp.broadcast_to(irv[...], (8, tok)).T[:, 0:1]
    mixed = co[toks(me)].astype(F32) + root * (gained - nhat * stat)
    mix_t[...] = mixed.T.astype(BF16)

    def blocks(k):
        to = lax.rem(me + k, n)
        return send(mix_t.at[slabs(to)], got.at[me], ms, mr.at[k], {"sp": to})

    def start_blocks(k, _):
        blocks(k).start()
        return 0

    d_state = jnp.dot(mixed.astype(BF16), omv[...], preferred_element_type=F32)
    here = keep[...]
    after = jnp.where(spot < tok - 1, pltpu.roll(here, tok - 1, 0), 1.0)
    a, b = scan_rows(after, d_state, True)
    enters[me] = jnp.broadcast_to(here[0:1] * b[0:1], (8, chan))
    cum[...] = a
    loc[...] = b

    def entering(k):
        to = lax.rem(me + k, n)
        return send(enters.at[me], enters.at[me], es, er.at[k], {"sp": to})

    def start_enter(k, _):
        entering(k).start()
        return 0

    lax.fori_loop(1, n, start_enter, 0)
    lax.fori_loop(1, n, start_blocks, 0)
    gow[...] = jnp.dot(mix_t[slabs(me)], hid_all[me], preferred_element_type=F32)

    def take_hidden(k, _):
        s = lax.rem(me - k + n, n)
        send(hid, hid_all.at[s], hs, hr.at[k], {"sp": s}).wait_recv()
        return 0

    def take_enter(k, _):
        s = lax.rem(me - k + n, n)
        send(enters.at[s], enters.at[s], es, er.at[k], {"sp": s}).wait_recv()
        return 0

    lax.fori_loop(1, n, take_enter, 0)
    enter = jnp.zeros((1, chan), F32)
    for s in range(n - 1, -1, -1):
        enter = jnp.where(s > me, carry[s, 0:1] * enter + enters[s, 0:1], enter)
    total = loc[...] + cum[...] * enter
    inward, opened, held, kept = scin[...], admit[...], retain[...], keep[...]
    signal = riv[...].astype(F32)
    g_rec[...] = total * inward * opened
    g_in[...] = total * inward * signal * opened * (1.0 - opened)
    d_log = total * prev[...] * kept - total * opened * signal * kept * kept / inward
    g_dec[...] = d_log * (-8.0 * speed) * held * (1.0 - held)

    lax.fori_loop(1, n, take_hidden, 0)

    def add(k, _):
        s = lax.rem(me - k + n, n)
        send(got.at[s], got.at[s], ms, mr.at[k], {"sp": s}).wait_recv()
        gow[...] += jnp.dot(got[s], hid_all[s], preferred_element_type=F32)
        return 0

    lax.fori_loop(1, n, add, 0)

    def flush(s, _):
        for i, o in arrays:
            @pl.when(jnp.logical_and(s <= z, z + 1 < zn))
            def _():
                line(i, o, s, True).wait_send()

            @pl.when(jnp.logical_and(s >= z, z > 0))
            def _():
                line(i, o, s, False).wait_send()

        return 0

    lax.fori_loop(0, zn, flush, 0)
    for i, o in arrays:
        part = o.at[pl.ds(0, (zn - 1) * tok), pl.ds(0, (m - 1) * q)]
        send(part, part, xs.at[i], f1r.at[i, 0], {"tp": lax.rem(j + 1, m)}).wait_send()
        part = o.at[pl.ds(0, zn * tok)]
        send(part, part, ds.at[i], dr.at[i, 0], {"sp": partner}).wait_send()
    to = {"sp": partner}
    others = pl.ds(0, n - 1)
    send(info.at[others], info.at[others], ns, nr.at[0], to).wait_send()
    send(carry.at[others], carry.at[others], cs, cr.at[0], to).wait_send()
    send(enters.at[others], enters.at[others], es, er.at[0], to).wait_send()
    send(hid_all.at[others], hid_all.at[others], hs, hr.at[0], to).wait_send()
    send(got.at[others], got.at[others], ms, mr.at[0], to).wait_send()
    part = red.at[pl.ds(0, (n - 1) * cap)]
    send(part, part, bs, br.at[0], to).wait_send()


def place_kernel(*refs):
    count = len(refs) // 2
    sems = refs[-1]
    copies = [
        pltpu.make_async_copy(refs[at], refs[count + at], sems.at[at]) for at in range(count)
    ]
    for c in copies:
        c.start()
    for c in copies:
        c.wait()


def vmem_limit(outs, scratch):
    total = 0
    held = [(s.shape, s.dtype) for s in scratch if s.dtype in (F32, BF16, jnp.int32)]
    for shape, kind in list(outs) + held:
        size = -(-shape[-1] // 128) * 128 * -(-shape[-2] // 8) * 8 * jnp.dtype(kind).itemsize
        for d in shape[:-2]:
            size *= d
        total += size
    return min(VMEM_LIMIT, total + SPARE)


def shards(
    cotangent,
    normed,
    inverse_root_mean_square,
    expert_norm_scale,
    routes,
    route_probability_weight,
    gate_weight,
    up_weight,
    down_weight,
    recurrence_input,
    recurrence_gate_logits,
    input_gate_logits,
    channel_decay_weight,
    extra_log_decay,
    output_matrix,
):
    tok, feats = normed.shape
    n, m = lax.axis_size("sp"), lax.axis_size("tp")
    picks = routes.shape[1]
    cap = 2 * picks * tok // n
    slots = n * cap
    q = feats // m
    ff = gate_weight.shape[2]
    chan = recurrence_input.shape[1]
    zn = n // 2
    dma = pltpu.SemaphoreType.DMA
    vmem = lambda *s: pltpu.VMEM(s, F32)
    half = lambda *s: pltpu.VMEM(s, BF16)
    outs = [
        ((1, feats, ff), BF16),
        ((1, feats, ff), BF16),
        ((1, ff, feats), BF16),
        ((feats // n, chan), F32),
        ((tok, chan), F32),
        ((tok, chan), F32),
        ((tok, chan), F32),
    ]
    scratch = [
        half(n * tok, feats),
        half(n * tok, feats),
        pltpu.VMEM((picks, tok), jnp.int32),
        vmem(picks, tok),
        vmem(1, tok),
        vmem(1, feats),
        half(tok, chan),
        half(tok, chan),
        half(tok, chan),
        vmem(1, chan),
        vmem(tok, chan),
        half(feats, chan),
        half(feats, ff),
        half(feats, ff),
        half(ff, feats),
        vmem(n, 8, tok),
        vmem(tok, chan),
        vmem(tok, chan),
        vmem(tok, chan),
        vmem(tok, chan),
        vmem(tok, chan),
        vmem(tok, chan),
        vmem(tok, chan),
        half(tok, chan),
        vmem(n, 8, chan),
        vmem(n, 8, chan),
        half(slots, feats),
        half(slots, feats),
        half(slots, ff),
        half(slots, ff),
        half(slots, ff),
        half(slots, feats),
        half(m - 1, slots, q),
        half(slots, q),
        half(slots, q),
        half(tok, feats),
        half(n, tok, chan),
        half(feats, tok),
        half(n, feats // n, tok),
        dma((15,)),
        dma((2, 2, zn)),
        dma((2, zn)),
        dma((2,)),
        dma((2, zn)),
        dma((2, zn)),
        dma((2,)),
        dma((2, zn)),
        dma,
        dma((n,)),
        dma,
        dma((n,)),
        dma,
        dma((n,)),
        dma((zn,)),
        dma((zn,)),
        dma,
        dma((n,)),
        dma((m,)),
        dma((m,)),
        dma,
        dma((n,)),
        dma,
        dma((n,)),
    ]
    args = (
        normed,
        cotangent,
        routes.T,
        route_probability_weight.T,
        inverse_root_mean_square[None, :],
        expert_norm_scale[None, :],
        recurrence_input,
        recurrence_gate_logits,
        input_gate_logits,
        channel_decay_weight[None, :],
        extra_log_decay,
        output_matrix,
        gate_weight,
        up_weight,
        down_weight,
    )
    args = [pltpu.with_memory_space_constraint(a, pltpu.HBM) for a in args]
    results = pl.pallas_call(
        functools.partial(block_kernel, n, m),
        out_shape=tuple(jax.ShapeDtypeStruct(s, d) for s, d in outs),
        in_specs=[pl.BlockSpec(memory_space=pltpu.HBM)] * len(args),
        out_specs=tuple(pl.BlockSpec(memory_space=pltpu.VMEM) for _ in outs),
        scratch_shapes=scratch,
        compiler_params=pltpu.CompilerParams(
            collective_id=0, has_side_effects=True, vmem_limit_bytes=vmem_limit(outs, scratch)
        ),
    )(*args)
    return pl.pallas_call(
        place_kernel,
        out_shape=tuple(jax.ShapeDtypeStruct(s, d) for s, d in outs),
        in_specs=[pl.BlockSpec(memory_space=pltpu.VMEM)] * len(outs),
        out_specs=tuple(pl.BlockSpec(memory_space=pltpu.HBM) for _ in outs),
        scratch_shapes=[dma((len(outs),))],
        compiler_params=pltpu.CompilerParams(vmem_limit_bytes=LEAST),
    )(*results)


def solution(mesh):
    return jax.shard_map(
        shards,
        mesh=mesh,
        in_specs=(
            P("sp", None),
            P("sp", None),
            P("sp"),
            P(),
            P("sp", None),
            P("sp", None),
            P("sp", None, "tp"),
            P("sp", None, "tp"),
            P("sp", "tp", None),
            P("sp", "tp"),
            P("sp", "tp"),
            P("sp", "tp"),
            P("tp"),
            P("sp", "tp"),
            P(None, "tp"),
        ),
        out_specs=(
            P("sp", None, "tp"),
            P("sp", None, "tp"),
            P("sp", "tp", None),
            P("sp", "tp"),
            P("sp", "tp"),
            P("sp", "tp"),
            P("sp", "tp"),
        ),
        check_vma=False,
    )
```

```python
import functools

import jax
import jax.numpy as jnp
from jax import lax
from jax.experimental import pallas as pl
from jax.experimental.pallas import tpu as pltpu
from jax.sharding import PartitionSpec as P

MESH = pl.DeviceIdType.MESH
VMEM_LIMIT = 63 * 1024 * 1024
SPARE = 8 * 1024 * 1024
LEAST = 12 * 1024 * 1024
F32, BF16 = jnp.float32, jnp.bfloat16
ROWDIMS = (((0,), (0,)), ((), ()))
COLDIMS = (((1,), (1,)), ((), ()))


def sides(m):
    high = max(d for d in range(1, m + 1) if m % d == 0 and d * d <= m)
    return high, m // high


def greet(n, m, me, j):
    barrier = pltpu.get_barrier_semaphore()
    for k in range(1, n):
        pl.semaphore_signal(
            barrier, inc=1, device_id={"sp": lax.rem(me + k, n)}, device_id_type=MESH
        )
    for p in range(1, m):
        pl.semaphore_signal(
            barrier, inc=1, device_id={"tp": lax.rem(j + p, m)}, device_id_type=MESH
        )
    pl.semaphore_wait(barrier, n - 1 + m - 1)


def send(src, dst, send_sem, recv_sem, where):
    return pltpu.make_async_remote_copy(
        src_ref=src,
        dst_ref=dst,
        send_sem=send_sem,
        recv_sem=recv_sem,
        device_id=where,
        device_id_type=MESH,
    )


def scan_rows(a, b, reverse):
    rows = a.shape[0]
    place = lax.broadcasted_iota(jnp.int32, a.shape, 0)
    step = 1
    while step < rows:
        if reverse:
            known = place < rows - step
            shift = rows - step
        else:
            known = place >= step
            shift = step
        a_far = jnp.where(known, pltpu.roll(a, shift, 0), 1.0)
        b_far = jnp.where(known, pltpu.roll(b, shift, 0), 0.0)
        b = a * b_far + b
        a = a * a_far
        step *= 2
    return a, b


def softplus_of_negative(w):
    t = jnp.exp(-jnp.abs(w))
    series = jnp.zeros_like(t)
    for k in range(10, 0, -1):
        series = t * ((1.0 / k if k % 2 else -1.0 / k) + series)
    return jnp.maximum(-w, 0.0) + jnp.where(t < 0.1, series, jnp.log(1.0 + t))


def one_minus_exp(y):
    series = jnp.ones_like(y)
    for k in range(10, 1, -1):
        series = 1.0 + y * (1.0 / k) * series
    return jnp.where(y > -0.5, -y * series, 1.0 - jnp.exp(y))


def block_kernel(
    n, m,
    nrm, cot, routes, probs, irms, gain, rin, rgate, igate, decay, extra, omat, gw, uw, dw,
    ggate, gup, gdown, gow, g_rec, g_dec, g_in,
    xo, co, rtv, pbv, irv, gnv, riv, rgv, igv, dcv, exv, omv, gwv, uwv, dwv,
    info, keep, scin, admit, retain, cum, loc, prev, hid, carry, enters,
    xg, yg, act, dg, du, pr, st1, mid, st2, red, back, out, hid_all, mix_t, got,
    ld, zs, zr, xs, f1r, f2r, ds, dr, ns, nr, cs, cr, hs, hr, q1, r1, q2, r2, bs, br,
    gs, gr, ms, mr, us, ur, es, er,
):
    me, j = lax.axis_index("sp"), lax.axis_index("tp")
    tok, feats = nrm.shape
    slots = pr.shape[0]
    cap, q = slots // n, feats // m
    chan, ff = keep.shape[1], gwv.shape[1]
    zn = n // 2
    z, par = lax.div(me, 2), lax.rem(me, 2)
    partner = me + 1 - 2 * par
    high, low = sides(m)
    upper, lower = lax.div(j, low), lax.rem(j, low)
    toks = lambda s: pl.ds(pl.multiple_of(s * tok, tok), tok)
    rows = lambda s: pl.ds(pl.multiple_of(s * cap, cap), cap)
    rows2 = lambda s: pl.ds(pl.multiple_of(s * 2 * cap, 2 * cap), 2 * cap)
    cols = lambda t: pl.ds(pl.multiple_of(t * q, q), q)
    arrays = ((0, xo), (1, co))

    def size(i):
        return low if i == 0 else high

    def near(i, along, across):
        up, down = (across, along) if i == 0 else (along, across)
        return lax.rem(upper + up, high) * low + lax.rem(lower + down, low)

    def source(k):
        fewer = jnp.minimum(z, zn - 1 - z)
        paired = k <= 2 * fewer
        d = jnp.where(paired, lax.div(k + 1, 2), k - fewer)
        odd = lax.rem(k, 2)
        down = jnp.where(paired, odd, jnp.where(z > zn - 1 - z, 1, 0))
        return z + d - 2 * d * down

    loads = [
        pltpu.make_async_copy(src, dst, ld.at[at])
        for at, (src, dst) in enumerate(
            (
                (routes, rtv),
                (probs, pbv),
                (nrm, xo.at[toks(me)]),
                (cot, co.at[toks(me)]),
                (rgate, rgv),
                (decay, dcv),
                (extra, exv),
                (igate, igv),
                (rin, riv),
                (gw.at[0], gwv),
                (uw.at[0], uwv),
                (dw.at[0], dwv),
                (omat, omv),
                (gain, gnv),
                (irms, irv),
            )
        )
    ]
    for c in loads:
        c.start()
    greet(n, m, me, j)
    loads[0].wait()
    loads[1].wait()
    info[me] = jnp.concatenate(
        [rtv[...].astype(F32), pbv[...], jnp.zeros((4, tok), F32)], axis=0
    )

    def told(k):
        to = lax.rem(me + k, n)
        return send(info.at[me], info.at[me], ns, nr.at[me], {"sp": to})

    def tell(k, _):
        told(k).start()
        return 0

    lax.fori_loop(1, n, tell, 0)

    loads[2].wait()
    loads[3].wait()

    def line(i, o, s, up):
        block = o.at[toks(2 * s + par), cols(j)]
        to = me + 2 if up else me - 2
        return send(block, block, zs.at[i, int(up), s], zr.at[i, s], {"sp": to})

    for i, o in arrays:
        @pl.when(z + 1 < zn)
        def _():
            line(i, o, z, True).start()

        @pl.when(z > 0)
        def _():
            line(i, o, z, False).start()

    def across(i, o, s):
        block = o.at[toks(2 * s + par)]
        return send(block, block, ds.at[i], dr.at[i, s], {"sp": partner})

    for i, o in arrays:
        across(i, o, z).start()

    for at in range(4, 9):
        loads[at].wait()
    speed = softplus_of_negative(dcv[...])
    retain[...] = jax.nn.sigmoid(rgv[...].astype(F32))
    admit[...] = jax.nn.sigmoid(igv[...].astype(F32))
    log_keep = -8.0 * retain[...] * speed + exv[...]
    keep[...] = jnp.exp(log_keep)
    scin[...] = jnp.sqrt(one_minus_exp(2.0 * log_keep))
    a, b = scan_rows(keep[...], scin[...] * admit[...] * riv[...].astype(F32), False)
    cum[...] = a
    loc[...] = b
    carry[me] = jnp.concatenate(
        [a[tok - 1 : tok], b[tok - 1 : tok], jnp.zeros((6, chan), F32)], axis=0
    )

    def carried(k):
        to = lax.rem(me + k, n)
        return send(carry.at[me], carry.at[me], cs, cr.at[k], {"sp": to})

    def start_carry(k, _):
        carried(k).start()
        return 0

    lax.fori_loop(1, n, start_carry, 0)

    earlier = (
        lax.broadcasted_iota(jnp.int32, (tok, tok), 0)
        < lax.broadcasted_iota(jnp.int32, (tok, tok), 1)
    ).astype(F32).astype(BF16)

    def place(s):
        @pl.when(s != me)
        def _():
            send(info.at[s], info.at[s], ns, nr.at[s], {"sp": s}).wait_recv()

        mine = info[s]
        first, second = mine[0:1] == me.astype(F32), mine[1:2] == me.astype(F32)
        member = jnp.where(jnp.logical_or(first, second), 1.0, 0.0)
        wide = jnp.broadcast_to(member, (8, tok))
        ranking = jnp.dot(wide.astype(BF16), earlier, preferred_element_type=F32)
        weight = jnp.where(first, mine[2:3], 0.0) + jnp.where(second, mine[3:4], 0.0)
        return jnp.where(member > 0.0, ranking[0:1], -1.0), weight

    for at in range(9, 15):
        loads[at].wait()

    def onward(s, i, o):
        block = o.at[toks(2 * s + par), cols(j)]
        for p in range(1, size(i)):
            send(block, block, xs.at[i], f1r.at[i, s], {"tp": near(i, p, 0)}).start()
        for p in range(1, size(1 - i)):
            send(block, block, xs.at[i], f2r.at[i, s], {"tp": near(i, 0, p)}).start()

    def several(o, s, count):
        return o.at[toks(2 * s + par), pl.ds(0, count * q)]

    def relayed(s):
        for i, o in arrays:
            if size(i) > 1:
                part = several(o, s, size(i) - 1)
                send(part, part, xs.at[i], f1r.at[i, s], {"tp": near(i, 1, 0)}).wait_recv()
            for c in range(1, size(i)):
                block = o.at[toks(2 * s + par), cols(near(i, size(i) - c, 0))]
                for p in range(1, size(1 - i)):
                    send(block, block, xs.at[i], f2r.at[i, s], {"tp": near(i, 0, p)}).start()

    def whole(s):
        for i, o in arrays:
            if size(1 - i) > 1:
                part = several(o, s, m - size(i))
                send(part, part, xs.at[i], f2r.at[i, s], {"tp": near(i, 0, 1)}).wait_recv()
            across(i, o, s).start()

    span = min(feats, 512)
    unit = min(ff, 256)

    def compute(s):
        other = 2 * s + 1 - par
        for i, o in arrays:
            block = o.at[toks(other)]
            send(block, block, ds.at[i], dr.at[i, s], {"sp": partner}).wait_recv()
        (low_at, low_weight), (high_at, high_weight) = place(2 * s), place(2 * s + 1)
        high_at = jnp.where(high_at >= 0.0, high_at + float(cap), -1.0)
        at = jnp.concatenate([low_at, high_at], axis=1)
        weight = jnp.concatenate([low_weight, high_weight], axis=1)
        here = lax.broadcasted_iota(jnp.int32, (2 * cap, 2 * tok), 0).astype(F32)
        hit = here == at
        one = jnp.where(hit, 1.0, 0.0)
        share = jnp.sum(jnp.where(hit, weight, 0.0), axis=1, keepdims=True)
        one = one.astype(BF16)
        pair = pl.ds(pl.multiple_of(s * 2 * tok, 2 * tok), 2 * tok)
        land = rows2(s)
        for t in range(feats // span):
            f = pl.ds(t * span, span)
            xg[land, f] = jnp.dot(one, xo[pair, f], preferred_element_type=F32).astype(BF16)
            yg[land, f] = (share * jnp.dot(one, co[pair, f], preferred_element_type=F32)).astype(
                BF16
            )
        for t in range(ff // unit):
            f = pl.ds(t * unit, unit)
            gate = jnp.dot(xg[land, :], gwv[:, f], preferred_element_type=F32)
            up = jnp.dot(xg[land, :], uwv[:, f], preferred_element_type=F32)
            d_act = lax.dot_general(yg[land, :], dwv[f, :], COLDIMS, preferred_element_type=F32)
            sigma = jax.nn.sigmoid(gate)
            swish = gate * sigma
            act[land, f] = (swish * up).astype(BF16)
            dg[land, f] = (d_act * up * sigma * (1.0 + gate * (1.0 - sigma))).astype(BF16)
            du[land, f] = (d_act * swish).astype(BF16)
        for t in range(feats // span):
            f = pl.ds(t * span, span)
            part = lax.dot_general(dg[land, :], gwv[f, :], COLDIMS, preferred_element_type=F32)
            part += lax.dot_general(du[land, :], uwv[f, :], COLDIMS, preferred_element_type=F32)
            pr[land, f] = part.astype(BF16)

    parts = 2 if q % 256 == 0 else 1
    piece = lambda v: pl.ds(v * (q // parts), q // parts)

    def shipped(s, v):
        return send(
            red.at[rows(s), piece(v)], back.at[rows(me), piece(v)], bs, br.at[v, me], {"sp": s}
        )

    def half_sums(s):
        for h in range(2):
            for p in range(1, size(h)):
                for c in range(size(1 - h)):
                    send(
                        pr.at[rows(2 * s + h), cols(near(h, p, c))],
                        st1.at[h, p - 1, c, rows(s)],
                        q1.at[h],
                        r1.at[h, s],
                        {"tp": near(h, p, 0)},
                    ).start()

    def middle(s):
        for h in range(2):
            if size(h) > 1:
                part = st1.at[h, pl.ds(0, size(h) - 1), pl.ds(0, size(1 - h)), rows(s)]
                send(part, part, q1.at[h], r1.at[h, s], {"tp": near(h, 1, 0)}).wait_recv()
            for c in range(size(1 - h)):
                total = pr[rows(2 * s + h), cols(near(h, 0, c))].astype(F32)
                for p in range(1, size(h)):
                    total = total + st1[h, p - 1, c, rows(s)].astype(F32)
                mid[h, c, rows(s)] = total.astype(BF16)
            for c in range(1, size(1 - h)):
                send(
                    mid.at[h, c, rows(s)],
                    st2.at[h, c - 1, rows(s)],
                    q2.at[h],
                    r2.at[h, s],
                    {"tp": near(h, 0, c)},
                ).start()

    def reduce(s):
        for h in range(2):
            if size(1 - h) > 1:
                part = st2.at[h, pl.ds(0, size(1 - h) - 1), rows(s)]
                send(part, part, q2.at[h], r2.at[h, s], {"tp": near(h, 0, 1)}).wait_recv()
            total = mid[h, 0, rows(s)].astype(F32)
            for c in range(1, size(1 - h)):
                total = total + st2[h, c - 1, rows(s)].astype(F32)
            red[rows(2 * s + h)] = total.astype(BF16)
        for v in range(parts):
            for h in range(2):
                @pl.when(2 * s + h != me)
                def _():
                    shipped(2 * s + h, v).start()

    spot = lax.broadcasted_iota(jnp.int32, (tok, chan), 0)

    def hidden():
        def take_carry(k, _):
            s = lax.rem(me - k + n, n)
            send(carry.at[s], carry.at[s], cs, cr.at[k], {"sp": s}).wait_recv()
            return 0

        lax.fori_loop(1, n, take_carry, 0)
        state = jnp.zeros((1, chan), F32)
        for s in range(n):
            state = jnp.where(s < me, carry[s, 0:1] * state + carry[s, 1:2], state)
        states = loc[...] + cum[...] * state
        hid[...] = states.astype(BF16)
        prev[...] = jnp.where(spot >= 1, pltpu.roll(states, 1, 0), state)
        hid_all[me] = hid[...]

    def share_hidden(k, _):
        to = lax.rem(me + k, n)
        send(hid, hid_all.at[me], hs, hr.at[k], {"sp": to}).start()
        return 0


    def passing(s):
        return jnp.where(s < z, jnp.where(z + 1 < zn, 1, 0), jnp.where(z > 0, 1, 0))

    def take_line(s, i, o):
        line(i, o, s, True).wait_recv()

        @pl.when(jnp.logical_and(s < z, z + 1 < zn))
        def _():
            line(i, o, s, True).start()

        @pl.when(jnp.logical_and(s > z, z > 0))
        def _():
            line(i, o, s, False).start()

    compute(z)

    def gather(k, _):
        s = source(k)
        passes = passing(s)
        late = jnp.logical_and(k >= 3, passes == 1)

        @pl.when(jnp.logical_and(k >= 3, passes == 0))
        def _():
            relayed(source(k - 2))

        for i, o in arrays:
            take_line(s, i, o)

            @pl.when(jnp.logical_not(late))
            def _():
                onward(s, i, o)

        @pl.when(late)
        def _():
            relayed(source(k - 2))

            @pl.when(k == zn - 1)
            def _():
                relayed(source(k - 1))

            for i, o in arrays:
                onward(s, i, o)

        return 0

    lax.fori_loop(1, zn, gather, 0)
    hidden()

    @pl.when(passing(source(zn - 1)) == 0)
    def _():
        relayed(source(zn - 2))

    def middles(g, _):
        middle(source(g))
        return 0

    def reduces(g, _):
        reduce(source(g))
        return 0

    def experts(k, _):
        @pl.when(k > 1)
        def _():
            whole(source(k - 1))

        @pl.when(k == zn - 1)
        def _():
            relayed(source(k))

            def early(g, _):
                half_sums(source(g))
                return 0

            lax.fori_loop(0, zn - 2, early, 0)

        @pl.when(k == zn)
        def _():
            lax.fori_loop(1, n, share_hidden, 0)

        @pl.when(k > 1)
        def _():
            compute(source(k - 1))

        @pl.when(k == zn)
        def _():
            lax.fori_loop(0, zn - 2, middles, 0)

        @pl.when(k >= zn - 1)
        def _():
            half_sums(source(k - 1))

        return 0

    lax.fori_loop(1, zn + 1, experts, 0)
    middle(source(zn - 2))

    def wide_grads(t, _):
        f = pl.ds(pl.multiple_of(t * 256, 256), 256)
        rowsof = xg[:, f]
        ggate[0, f, :] = lax.dot_general(
            rowsof, dg[...], ROWDIMS, preferred_element_type=F32
        ).astype(BF16)
        gup[0, f, :] = lax.dot_general(
            rowsof, du[...], ROWDIMS, preferred_element_type=F32
        ).astype(BF16)
        return 0

    lax.fori_loop(0, zn - 2, reduces, 0)
    for t in range(ff // min(ff, 128)):
        f = pl.ds(t * min(ff, 128), min(ff, 128))
        gdown[0, f, :] = lax.dot_general(
            act[:, f], yg[...], ROWDIMS, preferred_element_type=F32
        ).astype(BF16)
    lax.fori_loop(0, feats // 512, wide_grads, 0)
    reduce(source(zn - 2))
    middle(source(zn - 1))
    lax.fori_loop(feats // 512, feats // 256, wide_grads, 0)
    reduce(source(zn - 1))
    back[rows(me)] = red[rows(me)]

    own = info[me]
    experts = lax.broadcasted_iota(jnp.int32, (n, tok), 0).astype(F32)
    member = jnp.where(jnp.logical_or(own[0:1] == experts, own[1:2] == experts), 1.0, 0.0)
    ranking = jnp.dot(member.astype(BF16), earlier, preferred_element_type=F32)
    ranking = jnp.where(member > 0.0, ranking, -1.0)
    depth = lax.broadcasted_iota(jnp.int32, (n, cap, tok), 1).astype(F32)
    pick = jnp.where(depth == ranking[:, None, :], 1.0, 0.0).reshape(slots, tok).astype(BF16)

    for v in range(parts):
        def collect(k, _):
            s = lax.rem(me - k + n, n)
            block = back.at[rows(s), piece(v)]
            send(block, block, bs, br.at[v, s], {"sp": s}).wait_recv()
            return 0

        lax.fori_loop(1, n, collect, 0)
        total = lax.dot_general(pick, back[:, piece(v)], ROWDIMS, preferred_element_type=F32)
        spread = q // parts
        fields = lambda t: pl.ds(pl.multiple_of(t * q + v * spread, spread), spread)
        out[:, fields(j)] = total.astype(BF16)
        mine = out.at[:, fields(j)]
        for p in range(1, m):
            send(mine, mine, gs.at[p], gr.at[v, p], {"tp": lax.rem(j + p, m)}).start()
    for v in range(parts):
        spread = q // parts
        fields = lambda t: pl.ds(pl.multiple_of(t * q + v * spread, spread), spread)
        for p in range(1, m):
            far = lax.rem(j - p + m, m)
            theirs = out.at[:, fields(far)]
            send(theirs, theirs, gs.at[p], gr.at[v, p], {"tp": far}).wait_recv()
    mine = out.at[:, cols(j)]
    for p in range(1, m):
        send(mine, mine, gs.at[p], gr.at[0, p], {"tp": lax.rem(j + p, m)}).wait_send()

    slab = feats // n
    slabs = lambda s: pl.ds(pl.multiple_of(s * slab, slab), slab)
    scale = gnv[...]
    nhat = xo[toks(me)].astype(F32) / scale
    gained = scale * out[...].astype(F32)
    stat = jnp.mean(gained * nhat, axis=1, keepdims=True)
    root = jnp.broadcast_to(irv[...], (8, tok)).T[:, 0:1]
    mixed = co[toks(me)].astype(F32) + root * (gained - nhat * stat)
    mix_t[...] = mixed.T.astype(BF16)

    def share_of(i):
        part = slab // size(i)
        return pl.ds(pl.multiple_of((lower if i == 0 else upper) * part, part), part)

    def start_blocks(i):
        part = slab // size(i)
        own = lower if i == 0 else upper

        def start(k, _):
            to = lax.rem(me + k, n)
            piece = pl.ds(pl.multiple_of(to * slab + own * part, part), part)
            send(
                mix_t.at[piece], got.at[me, share_of(i)], ms, mr.at[me], {"sp": to}
            ).start()
            return 0

        lax.fori_loop(1, n, start, 0)

    def pass_block(i, s):
        block = got.at[s, share_of(i)]
        send(block, block, ms, mr.at[s], {"sp": s}).wait_recv()
        for p in range(1, size(i)):
            send(block, block, us.at[i], ur.at[s], {"tp": near(i, p, 0)}).start()

    def end_block(i, s):
        if size(i) > 1:
            block = got.at[s, pl.ds(0, slab // size(i) * (size(i) - 1))]
            send(block, block, us.at[i], ur.at[s], {"tp": near(i, 1, 0)}).wait_recv()
        gow[...] += jnp.dot(got[s], hid_all[s], preferred_element_type=F32)

    def on_side(work, s):
        @pl.when(lax.rem(s, 2) == 0)
        def _():
            work(0, s)

        @pl.when(lax.rem(s, 2) == 1)
        def _():
            work(1, s)

    d_state = jnp.dot(mixed.astype(BF16), omv[...], preferred_element_type=F32)
    here = keep[...]
    after = jnp.where(spot < tok - 1, pltpu.roll(here, tok - 1, 0), 1.0)
    a, b = scan_rows(after, d_state, True)
    enters[me] = jnp.broadcast_to(here[0:1] * b[0:1], (8, chan))
    cum[...] = a
    loc[...] = b

    def entering(k):
        to = lax.rem(me + k, n)
        return send(enters.at[me], enters.at[me], es, er.at[k], {"sp": to})

    def start_enter(k, _):
        entering(k).start()
        return 0

    lax.fori_loop(1, n, start_enter, 0)
    @pl.when(par == 0)
    def _():
        start_blocks(0)

    @pl.when(par == 1)
    def _():
        start_blocks(1)

    gow[...] = jnp.dot(mix_t[slabs(me)], hid_all[me], preferred_element_type=F32)

    def take_hidden(k, _):
        s = lax.rem(me - k + n, n)
        send(hid, hid_all.at[s], hs, hr.at[k], {"sp": s}).wait_recv()
        return 0

    def nearby(k):
        return 2 * source(lax.div(k, 2)) + lax.rem(k + par, 2)

    def pass_blocks(k, _):
        on_side(pass_block, nearby(k))
        return 0

    def end_blocks(k, _):
        on_side(end_block, nearby(k))
        return 0

    lax.fori_loop(1, n, pass_blocks, 0)

    def take_enter(k, _):
        s = lax.rem(me - k + n, n)
        send(enters.at[s], enters.at[s], es, er.at[k], {"sp": s}).wait_recv()
        return 0

    lax.fori_loop(1, n, take_enter, 0)
    enter = jnp.zeros((1, chan), F32)
    for s in range(n - 1, -1, -1):
        enter = jnp.where(s > me, carry[s, 0:1] * enter + enters[s, 0:1], enter)
    total = loc[...] + cum[...] * enter
    inward, opened, held, kept = scin[...], admit[...], retain[...], keep[...]
    signal = riv[...].astype(F32)
    g_rec[...] = total * inward * opened
    g_in[...] = total * inward * signal * opened * (1.0 - opened)
    d_log = total * prev[...] * kept - total * opened * signal * kept * kept / inward
    g_dec[...] = d_log * (-8.0 * speed) * held * (1.0 - held)

    lax.fori_loop(1, n, take_hidden, 0)

    lax.fori_loop(1, n, end_blocks, 0)

    def flush(s, _):
        for i, o in arrays:
            @pl.when(jnp.logical_and(s <= z, z + 1 < zn))
            def _():
                line(i, o, s, True).wait_send()

            @pl.when(jnp.logical_and(s >= z, z > 0))
            def _():
                line(i, o, s, False).wait_send()

        return 0

    lax.fori_loop(0, zn, flush, 0)
    for i, o in arrays:
        part = o.at[pl.ds(0, (zn - 1) * tok), pl.ds(0, (m - 1) * q)]
        send(part, part, xs.at[i], f1r.at[i, 0], {"tp": lax.rem(j + 1, m)}).wait_send()
        part = o.at[pl.ds(0, zn * tok)]
        send(part, part, ds.at[i], dr.at[i, 0], {"sp": partner}).wait_send()
    for h in range(2):
        if size(h) > 1:
            part = st1.at[h, pl.ds(0, size(h) - 1), pl.ds(0, size(1 - h))]
            send(part, part, q1.at[h], r1.at[h, 0], {"tp": near(h, 1, 0)}).wait_send()
        if size(1 - h) > 1:
            part = st2.at[h, pl.ds(0, size(1 - h) - 1)]
            send(part, part, q2.at[h], r2.at[h, 0], {"tp": near(h, 0, 1)}).wait_send()
    to = {"sp": partner}
    others = pl.ds(0, n - 1)
    send(info.at[others], info.at[others], ns, nr.at[0], to).wait_send()
    send(carry.at[others], carry.at[others], cs, cr.at[0], to).wait_send()
    send(enters.at[others], enters.at[others], es, er.at[0], to).wait_send()
    send(hid_all.at[others], hid_all.at[others], hs, hr.at[0], to).wait_send()

    def flush_blocks(i):
        part = slab // size(i)
        block = got.at[others, pl.ds(0, part)]
        send(block, block, ms, mr.at[0], to).wait_send()

    @pl.when(par == 0)
    def _():
        flush_blocks(0)

    @pl.when(par == 1)
    def _():
        flush_blocks(1)

    for i in range(2):
        if size(i) > 1:
            part = slab // size(i) * (size(i) - 1)
            half_of = got.at[pl.ds(0, zn), pl.ds(0, part)]
            less = got.at[pl.ds(0, zn - 1), pl.ds(0, part)]

            @pl.when(par == i)
            def _():
                send(less, less, us.at[i], ur.at[0], {"tp": near(i, 1, 0)}).wait_send()

            @pl.when(par != i)
            def _():
                send(half_of, half_of, us.at[i], ur.at[0], {"tp": near(i, 1, 0)}).wait_send()

    part = red.at[pl.ds(0, (n - 1) * cap)]
    send(part, part, bs, br.at[0, 0], to).wait_send()


def place_kernel(*refs):
    count = len(refs) // 2
    sems = refs[-1]
    copies = [
        pltpu.make_async_copy(refs[at], refs[count + at], sems.at[at]) for at in range(count)
    ]
    for c in copies:
        c.start()
    for c in copies:
        c.wait()


def vmem_limit(outs, scratch):
    total = 0
    held = [(s.shape, s.dtype) for s in scratch if s.dtype in (F32, BF16, jnp.int32)]
    for shape, kind in list(outs) + held:
        size = -(-shape[-1] // 128) * 128 * -(-shape[-2] // 8) * 8 * jnp.dtype(kind).itemsize
        for d in shape[:-2]:
            size *= d
        total += size
    return min(VMEM_LIMIT, total + SPARE)


def shards(
    cotangent,
    normed,
    inverse_root_mean_square,
    expert_norm_scale,
    routes,
    route_probability_weight,
    gate_weight,
    up_weight,
    down_weight,
    recurrence_input,
    recurrence_gate_logits,
    input_gate_logits,
    channel_decay_weight,
    extra_log_decay,
    output_matrix,
):
    tok, feats = normed.shape
    n, m = lax.axis_size("sp"), lax.axis_size("tp")
    picks = routes.shape[1]
    cap = 2 * picks * tok // n
    slots = n * cap
    q = feats // m
    ff = gate_weight.shape[2]
    chan = recurrence_input.shape[1]
    zn = n // 2
    wide = max(sides(m))
    dma = pltpu.SemaphoreType.DMA
    vmem = lambda *s: pltpu.VMEM(s, F32)
    half = lambda *s: pltpu.VMEM(s, BF16)
    outs = [
        ((1, feats, ff), BF16),
        ((1, feats, ff), BF16),
        ((1, ff, feats), BF16),
        ((feats // n, chan), F32),
        ((tok, chan), F32),
        ((tok, chan), F32),
        ((tok, chan), F32),
    ]
    scratch = [
        half(n * tok, feats),
        half(n * tok, feats),
        pltpu.VMEM((picks, tok), jnp.int32),
        vmem(picks, tok),
        vmem(1, tok),
        vmem(1, feats),
        half(tok, chan),
        half(tok, chan),
        half(tok, chan),
        vmem(1, chan),
        vmem(tok, chan),
        half(feats, chan),
        half(feats, ff),
        half(feats, ff),
        half(ff, feats),
        vmem(n, 8, tok),
        vmem(tok, chan),
        vmem(tok, chan),
        vmem(tok, chan),
        vmem(tok, chan),
        vmem(tok, chan),
        vmem(tok, chan),
        vmem(tok, chan),
        half(tok, chan),
        vmem(n, 8, chan),
        vmem(n, 8, chan),
        half(slots, feats),
        half(slots, feats),
        half(slots, ff),
        half(slots, ff),
        half(slots, ff),
        half(slots, feats),
        half(2, max(wide - 1, 1), wide, zn * cap, q),
        half(2, wide, zn * cap, q),
        half(2, max(wide - 1, 1), zn * cap, q),
        half(slots, q),
        half(slots, q),
        half(tok, feats),
        half(n, tok, chan),
        half(feats, tok),
        half(n, feats // n, tok),
        dma((15,)),
        dma((2, 2, zn)),
        dma((2, zn)),
        dma((2,)),
        dma((2, zn)),
        dma((2, zn)),
        dma((2,)),
        dma((2, zn)),
        dma,
        dma((n,)),
        dma,
        dma((n,)),
        dma,
        dma((n,)),
        dma((2,)),
        dma((2, zn)),
        dma((2,)),
        dma((2, zn)),
        dma,
        dma((2, n)),
        dma((m,)),
        dma((2, m)),
        dma,
        dma((n,)),
        dma((2,)),
        dma((n,)),
        dma,
        dma((n,)),
    ]
    args = (
        normed,
        cotangent,
        routes.T,
        route_probability_weight.T,
        inverse_root_mean_square[None, :],
        expert_norm_scale[None, :],
        recurrence_input,
        recurrence_gate_logits,
        input_gate_logits,
        channel_decay_weight[None, :],
        extra_log_decay,
        output_matrix,
        gate_weight,
        up_weight,
        down_weight,
    )
    args = [pltpu.with_memory_space_constraint(a, pltpu.HBM) for a in args]
    results = pl.pallas_call(
        functools.partial(block_kernel, n, m),
        out_shape=tuple(jax.ShapeDtypeStruct(s, d) for s, d in outs),
        in_specs=[pl.BlockSpec(memory_space=pltpu.HBM)] * len(args),
        out_specs=tuple(pl.BlockSpec(memory_space=pltpu.VMEM) for _ in outs),
        scratch_shapes=scratch,
        compiler_params=pltpu.CompilerParams(
            collective_id=0, has_side_effects=True, vmem_limit_bytes=vmem_limit(outs, scratch)
        ),
    )(*args)
    return pl.pallas_call(
        place_kernel,
        out_shape=tuple(jax.ShapeDtypeStruct(s, d) for s, d in outs),
        in_specs=[pl.BlockSpec(memory_space=pltpu.VMEM)] * len(outs),
        out_specs=tuple(pl.BlockSpec(memory_space=pltpu.HBM) for _ in outs),
        scratch_shapes=[dma((len(outs),))],
        compiler_params=pltpu.CompilerParams(vmem_limit_bytes=LEAST),
    )(*results)


def solution(mesh):
    return jax.shard_map(
        shards,
        mesh=mesh,
        in_specs=(
            P("sp", None),
            P("sp", None),
            P("sp"),
            P(),
            P("sp", None),
            P("sp", None),
            P("sp", None, "tp"),
            P("sp", None, "tp"),
            P("sp", "tp", None),
            P("sp", "tp"),
            P("sp", "tp"),
            P("sp", "tp"),
            P("tp"),
            P("sp", "tp"),
            P(None, "tp"),
        ),
        out_specs=(
            P("sp", None, "tp"),
            P("sp", None, "tp"),
            P("sp", "tp", None),
            P("sp", "tp"),
            P("sp", "tp"),
            P("sp", "tp"),
            P("sp", "tp"),
        ),
        check_vma=False,
    )
```

```python
import functools

import jax
import jax.numpy as jnp
from jax import lax
from jax.experimental import pallas as pl
from jax.experimental.pallas import tpu as pltpu
from jax.sharding import PartitionSpec as P

MESH = pl.DeviceIdType.MESH
VMEM_LIMIT = 63 * 1024 * 1024
SPARE = 8 * 1024 * 1024
LEAST = 12 * 1024 * 1024
F32, BF16 = jnp.float32, jnp.bfloat16
ROWDIMS = (((0,), (0,)), ((), ()))
COLDIMS = (((1,), (1,)), ((), ()))


def sides(m):
    high = max(d for d in range(1, m + 1) if m % d == 0 and d * d <= m)
    return high, m // high


def greet(n, m, me, j):
    barrier = pltpu.get_barrier_semaphore()
    for k in range(1, n):
        pl.semaphore_signal(
            barrier, inc=1, device_id={"sp": lax.rem(me + k, n)}, device_id_type=MESH
        )
    for p in range(1, m):
        pl.semaphore_signal(
            barrier, inc=1, device_id={"tp": lax.rem(j + p, m)}, device_id_type=MESH
        )
    pl.semaphore_wait(barrier, n - 1 + m - 1)


def send(src, dst, send_sem, recv_sem, where):
    return pltpu.make_async_remote_copy(
        src_ref=src,
        dst_ref=dst,
        send_sem=send_sem,
        recv_sem=recv_sem,
        device_id=where,
        device_id_type=MESH,
    )


def scan_rows(a, b, reverse):
    rows = a.shape[0]
    place = lax.broadcasted_iota(jnp.int32, a.shape, 0)
    step = 1
    while step < rows:
        if reverse:
            known = place < rows - step
            shift = rows - step
        else:
            known = place >= step
            shift = step
        a_far = jnp.where(known, pltpu.roll(a, shift, 0), 1.0)
        b_far = jnp.where(known, pltpu.roll(b, shift, 0), 0.0)
        b = a * b_far + b
        a = a * a_far
        step *= 2
    return a, b


def softplus_of_negative(w):
    t = jnp.exp(-jnp.abs(w))
    series = jnp.zeros_like(t)
    for k in range(10, 0, -1):
        series = t * ((1.0 / k if k % 2 else -1.0 / k) + series)
    return jnp.maximum(-w, 0.0) + jnp.where(t < 0.1, series, jnp.log(1.0 + t))


def one_minus_exp(y):
    series = jnp.ones_like(y)
    for k in range(10, 1, -1):
        series = 1.0 + y * (1.0 / k) * series
    return jnp.where(y > -0.5, -y * series, 1.0 - jnp.exp(y))


def block_kernel(
    n, m,
    nrm, cot, routes, probs, irms, gain, rin, rgate, igate, decay, extra, omat, gw, uw, dw,
    ggate, gup, gdown, gow, g_rec, g_dec, g_in,
    xo, co, rtv, pbv, irv, gnv, riv, rgv, igv, dcv, exv, omv, gwv, uwv, dwv,
    info, keep, scin, admit, retain, cum, loc, prev, hid, carry, enters,
    xg, yg, act, dg, du, pr, st1, mid, st2, red, back, out, hid_all, mix_t, got, stats, nh_t,
    ld, zs, zr, xs, f1r, f2r, ds, dr, ns, nr, cs, cr, hs, hr, q1, r1, q2, r2, bs, br,
    gs, gr, ms, mr, us, ur, es, er, ws, wr,
):
    me, j = lax.axis_index("sp"), lax.axis_index("tp")
    tok, feats = nrm.shape
    slots = pr.shape[0]
    cap, q = slots // n, feats // m
    chan, ff = keep.shape[1], gwv.shape[1]
    zn = n // 2
    z, par = lax.div(me, 2), lax.rem(me, 2)
    partner = me + 1 - 2 * par
    high, low = sides(m)
    upper, lower = lax.div(j, low), lax.rem(j, low)
    toks = lambda s: pl.ds(pl.multiple_of(s * tok, tok), tok)
    rows = lambda s: pl.ds(pl.multiple_of(s * cap, cap), cap)
    rows2 = lambda s: pl.ds(pl.multiple_of(s * 2 * cap, 2 * cap), 2 * cap)
    cols = lambda t: pl.ds(pl.multiple_of(t * q, q), q)
    arrays = ((0, xo), (1, co))

    def size(i):
        return low if i == 0 else high

    def near(i, along, across):
        up, down = (across, along) if i == 0 else (along, across)
        return lax.rem(upper + up, high) * low + lax.rem(lower + down, low)

    def source(k):
        fewer = jnp.minimum(z, zn - 1 - z)
        paired = k <= 2 * fewer
        d = jnp.where(paired, lax.div(k + 1, 2), k - fewer)
        odd = lax.rem(k, 2)
        down = jnp.where(paired, odd, jnp.where(z > zn - 1 - z, 1, 0))
        return z + d - 2 * d * down

    loads = [
        pltpu.make_async_copy(src, dst, ld.at[at])
        for at, (src, dst) in enumerate(
            (
                (routes, rtv),
                (probs, pbv),
                (nrm, xo.at[toks(me)]),
                (cot, co.at[toks(me)]),
                (rgate, rgv),
                (decay, dcv),
                (extra, exv),
                (igate, igv),
                (rin, riv),
                (gw.at[0], gwv),
                (uw.at[0], uwv),
                (dw.at[0], dwv),
                (omat, omv),
                (gain, gnv),
                (irms, irv),
            )
        )
    ]
    for c in loads:
        c.start()
    greet(n, m, me, j)
    loads[0].wait()
    loads[1].wait()
    info[me] = jnp.concatenate(
        [rtv[...].astype(F32), pbv[...], jnp.zeros((4, tok), F32)], axis=0
    )

    def told(k):
        to = lax.rem(me + k, n)
        return send(info.at[me], info.at[me], ns, nr.at[me], {"sp": to})

    def tell(k, _):
        told(k).start()
        return 0

    lax.fori_loop(1, n, tell, 0)

    loads[2].wait()
    loads[3].wait()

    def line(i, o, s, up):
        block = o.at[toks(2 * s + par), cols(j)]
        to = me + 2 if up else me - 2
        return send(block, block, zs.at[i, int(up), s], zr.at[i, s], {"sp": to})

    for i, o in arrays:
        @pl.when(z + 1 < zn)
        def _():
            line(i, o, z, True).start()

        @pl.when(z > 0)
        def _():
            line(i, o, z, False).start()

    def across(i, o, s):
        block = o.at[toks(2 * s + par)]
        return send(block, block, ds.at[i], dr.at[i, s], {"sp": partner})

    for i, o in arrays:
        across(i, o, z).start()

    for at in range(4, 9):
        loads[at].wait()
    speed = softplus_of_negative(dcv[...])
    retain[...] = jax.nn.sigmoid(rgv[...].astype(F32))
    admit[...] = jax.nn.sigmoid(igv[...].astype(F32))
    log_keep = -8.0 * retain[...] * speed + exv[...]
    keep[...] = jnp.exp(log_keep)
    scin[...] = jnp.sqrt(one_minus_exp(2.0 * log_keep))
    a, b = scan_rows(keep[...], scin[...] * admit[...] * riv[...].astype(F32), False)
    cum[...] = a
    loc[...] = b
    carry[me] = jnp.concatenate(
        [a[tok - 1 : tok], b[tok - 1 : tok], jnp.zeros((6, chan), F32)], axis=0
    )

    def carried(k):
        to = lax.rem(me + k, n)
        return send(carry.at[me], carry.at[me], cs, cr.at[k], {"sp": to})

    def start_carry(k, _):
        carried(k).start()
        return 0

    lax.fori_loop(1, n, start_carry, 0)

    earlier = (
        lax.broadcasted_iota(jnp.int32, (tok, tok), 0)
        < lax.broadcasted_iota(jnp.int32, (tok, tok), 1)
    ).astype(F32).astype(BF16)

    def place(s):
        @pl.when(s != me)
        def _():
            send(info.at[s], info.at[s], ns, nr.at[s], {"sp": s}).wait_recv()

        mine = info[s]
        first, second = mine[0:1] == me.astype(F32), mine[1:2] == me.astype(F32)
        member = jnp.where(jnp.logical_or(first, second), 1.0, 0.0)
        wide = jnp.broadcast_to(member, (8, tok))
        ranking = jnp.dot(wide.astype(BF16), earlier, preferred_element_type=F32)
        weight = jnp.where(first, mine[2:3], 0.0) + jnp.where(second, mine[3:4], 0.0)
        return jnp.where(member > 0.0, ranking[0:1], -1.0), weight

    for at in range(9, 15):
        loads[at].wait()

    def onward(s, i, o):
        block = o.at[toks(2 * s + par), cols(j)]
        for p in range(1, size(i)):
            send(block, block, xs.at[i], f1r.at[i, s], {"tp": near(i, p, 0)}).start()
        for p in range(1, size(1 - i)):
            send(block, block, xs.at[i], f2r.at[i, s], {"tp": near(i, 0, p)}).start()

    def several(o, s, count):
        return o.at[toks(2 * s + par), pl.ds(0, count * q)]

    def relayed(s):
        for i, o in arrays:
            if size(i) > 1:
                part = several(o, s, size(i) - 1)
                send(part, part, xs.at[i], f1r.at[i, s], {"tp": near(i, 1, 0)}).wait_recv()
            for c in range(1, size(i)):
                block = o.at[toks(2 * s + par), cols(near(i, size(i) - c, 0))]
                for p in range(1, size(1 - i)):
                    send(block, block, xs.at[i], f2r.at[i, s], {"tp": near(i, 0, p)}).start()

    def whole(s):
        for i, o in arrays:
            if size(1 - i) > 1:
                part = several(o, s, m - size(i))
                send(part, part, xs.at[i], f2r.at[i, s], {"tp": near(i, 0, 1)}).wait_recv()
            across(i, o, s).start()

    span = min(feats, 512)
    unit = min(ff, 256)

    def compute(s):
        other = 2 * s + 1 - par
        for i, o in arrays:
            block = o.at[toks(other)]
            send(block, block, ds.at[i], dr.at[i, s], {"sp": partner}).wait_recv()
        (low_at, low_weight), (high_at, high_weight) = place(2 * s), place(2 * s + 1)
        high_at = jnp.where(high_at >= 0.0, high_at + float(cap), -1.0)
        at = jnp.concatenate([low_at, high_at], axis=1)
        weight = jnp.concatenate([low_weight, high_weight], axis=1)
        here = lax.broadcasted_iota(jnp.int32, (2 * cap, 2 * tok), 0).astype(F32)
        hit = here == at
        one = jnp.where(hit, 1.0, 0.0)
        share = jnp.sum(jnp.where(hit, weight, 0.0), axis=1, keepdims=True)
        one = one.astype(BF16)
        pair = pl.ds(pl.multiple_of(s * 2 * tok, 2 * tok), 2 * tok)
        land = rows2(s)
        for t in range(feats // span):
            f = pl.ds(t * span, span)
            xg[land, f] = jnp.dot(one, xo[pair, f], preferred_element_type=F32).astype(BF16)
            yg[land, f] = (share * jnp.dot(one, co[pair, f], preferred_element_type=F32)).astype(
                BF16
            )
        for t in range(ff // unit):
            f = pl.ds(t * unit, unit)
            gate = jnp.dot(xg[land, :], gwv[:, f], preferred_element_type=F32)
            up = jnp.dot(xg[land, :], uwv[:, f], preferred_element_type=F32)
            d_act = lax.dot_general(yg[land, :], dwv[f, :], COLDIMS, preferred_element_type=F32)
            sigma = jax.nn.sigmoid(gate)
            swish = gate * sigma
            act[land, f] = (swish * up).astype(BF16)
            dg[land, f] = (d_act * up * sigma * (1.0 + gate * (1.0 - sigma))).astype(BF16)
            du[land, f] = (d_act * swish).astype(BF16)
        for t in range(feats // span):
            f = pl.ds(t * span, span)
            part = lax.dot_general(dg[land, :], gwv[f, :], COLDIMS, preferred_element_type=F32)
            part += lax.dot_general(du[land, :], uwv[f, :], COLDIMS, preferred_element_type=F32)
            pr[land, f] = part.astype(BF16)

    parts = 2 if q % 256 == 0 else 1
    piece = lambda v: pl.ds(v * (q // parts), q // parts)

    def shipped(s, v):
        return send(
            red.at[rows(s), piece(v)], back.at[rows(me), piece(v)], bs, br.at[v, me], {"sp": s}
        )

    def half_sums(s):
        for h in range(2):
            for p in range(1, size(h)):
                for c in range(size(1 - h)):
                    send(
                        pr.at[rows(2 * s + h), cols(near(h, p, c))],
                        st1.at[h, p - 1, c, rows(s)],
                        q1.at[h],
                        r1.at[h, s],
                        {"tp": near(h, p, 0)},
                    ).start()

    def middle(s):
        for h in range(2):
            if size(h) > 1:
                part = st1.at[h, pl.ds(0, size(h) - 1), pl.ds(0, size(1 - h)), rows(s)]
                send(part, part, q1.at[h], r1.at[h, s], {"tp": near(h, 1, 0)}).wait_recv()
            for c in range(size(1 - h)):
                total = pr[rows(2 * s + h), cols(near(h, 0, c))].astype(F32)
                for p in range(1, size(h)):
                    total = total + st1[h, p - 1, c, rows(s)].astype(F32)
                mid[h, c, rows(s)] = total.astype(BF16)
            for c in range(1, size(1 - h)):
                send(
                    mid.at[h, c, rows(s)],
                    st2.at[h, c - 1, rows(s)],
                    q2.at[h],
                    r2.at[h, s],
                    {"tp": near(h, 0, c)},
                ).start()

    def reduce(s):
        for h in range(2):
            if size(1 - h) > 1:
                part = st2.at[h, pl.ds(0, size(1 - h) - 1), rows(s)]
                send(part, part, q2.at[h], r2.at[h, s], {"tp": near(h, 0, 1)}).wait_recv()
            total = mid[h, 0, rows(s)].astype(F32)
            for c in range(1, size(1 - h)):
                total = total + st2[h, c - 1, rows(s)].astype(F32)
            red[rows(2 * s + h)] = total.astype(BF16)
        for v in range(parts):
            for h in range(2):
                @pl.when(2 * s + h != me)
                def _():
                    shipped(2 * s + h, v).start()

    spot = lax.broadcasted_iota(jnp.int32, (tok, chan), 0)

    def hidden():
        def take_carry(k, _):
            s = lax.rem(me - k + n, n)
            send(carry.at[s], carry.at[s], cs, cr.at[k], {"sp": s}).wait_recv()
            return 0

        lax.fori_loop(1, n, take_carry, 0)
        state = jnp.zeros((1, chan), F32)
        for s in range(n):
            state = jnp.where(s < me, carry[s, 0:1] * state + carry[s, 1:2], state)
        states = loc[...] + cum[...] * state
        hid[...] = states.astype(BF16)
        prev[...] = jnp.where(spot >= 1, pltpu.roll(states, 1, 0), state)
        hid_all[me] = hid[...]

    def share_hidden(k, _):
        to = lax.rem(me + k, n)
        send(hid, hid_all.at[me], hs, hr.at[k], {"sp": to}).start()
        return 0


    def passing(s):
        return jnp.where(s < z, jnp.where(z + 1 < zn, 1, 0), jnp.where(z > 0, 1, 0))

    def take_line(s, i, o):
        line(i, o, s, True).wait_recv()

        @pl.when(jnp.logical_and(s < z, z + 1 < zn))
        def _():
            line(i, o, s, True).start()

        @pl.when(jnp.logical_and(s > z, z > 0))
        def _():
            line(i, o, s, False).start()

    turn = jnp.where(jnp.logical_or(z == 0, z == zn - 1), 1, 2)

    def gather(k, _):
        s = source(k)
        passes = passing(s)
        late = jnp.logical_and(k >= 3, passes == 1)

        @pl.when(jnp.logical_and(k >= 3, passes == 0))
        def _():
            relayed(source(k - 2))

        for i, o in arrays:
            take_line(s, i, o)

            @pl.when(jnp.logical_not(late))
            def _():
                onward(s, i, o)

        @pl.when(late)
        def _():
            relayed(source(k - 2))

            @pl.when(k == zn - 1)
            def _():
                relayed(source(k - 1))

            for i, o in arrays:
                onward(s, i, o)

        @pl.when(k == turn)
        def _():
            compute(z)

        return 0

    lax.fori_loop(1, zn, gather, 0)
    hidden()

    @pl.when(passing(source(zn - 1)) == 0)
    def _():
        relayed(source(zn - 2))

    def middles(g, _):
        middle(source(g))
        return 0

    def reduces(g, _):
        reduce(source(g))
        return 0

    def experts(k, _):
        @pl.when(k > 1)
        def _():
            whole(source(k - 1))

        @pl.when(k == zn - 1)
        def _():
            relayed(source(k))

            def early(g, _):
                half_sums(source(g))
                return 0

            lax.fori_loop(0, zn - 2, early, 0)

        @pl.when(k == zn)
        def _():
            lax.fori_loop(1, n, share_hidden, 0)

        @pl.when(k > 1)
        def _():
            compute(source(k - 1))

        @pl.when(k == zn)
        def _():
            lax.fori_loop(0, zn - 2, middles, 0)

        @pl.when(k >= zn - 1)
        def _():
            half_sums(source(k - 1))

        return 0

    lax.fori_loop(1, zn + 1, experts, 0)
    middle(source(zn - 2))

    def wide_grads(t, _):
        f = pl.ds(pl.multiple_of(t * 256, 256), 256)
        rowsof = xg[:, f]
        ggate[0, f, :] = lax.dot_general(
            rowsof, dg[...], ROWDIMS, preferred_element_type=F32
        ).astype(BF16)
        gup[0, f, :] = lax.dot_general(
            rowsof, du[...], ROWDIMS, preferred_element_type=F32
        ).astype(BF16)
        return 0

    lax.fori_loop(0, zn - 2, reduces, 0)
    for t in range(ff // min(ff, 128)):
        f = pl.ds(t * min(ff, 128), min(ff, 128))
        gdown[0, f, :] = lax.dot_general(
            act[:, f], yg[...], ROWDIMS, preferred_element_type=F32
        ).astype(BF16)
    middle(source(zn - 1))
    lax.fori_loop(0, feats // 512, wide_grads, 0)
    reduce(source(zn - 2))
    reduce(source(zn - 1))
    back[rows(me)] = red[rows(me)]
    lax.fori_loop(feats // 512, feats // 256, wide_grads, 0)

    slab = feats // n
    slabs = lambda s: pl.ds(pl.multiple_of(s * slab, slab), slab)
    window = nh_t.shape[1]
    base = lax.div(me * slab, window)
    band = pl.ds(pl.multiple_of(base * window, window), window)
    inside = pl.ds(pl.multiple_of(me * slab - base * window, slab), slab)

    def turned(s, _):
        nh_t[s] = (xo[toks(s), band].astype(F32) / gnv[:, band]).T.astype(BF16)
        return 0

    lax.fori_loop(0, n, turned, 0)
    root = jnp.broadcast_to(irv[...], (8, tok)).T[:, 0:1]

    own = info[me]
    experts = lax.broadcasted_iota(jnp.int32, (n, tok), 0).astype(F32)
    member = jnp.where(jnp.logical_or(own[0:1] == experts, own[1:2] == experts), 1.0, 0.0)
    ranking = jnp.dot(member.astype(BF16), earlier, preferred_element_type=F32)
    ranking = jnp.where(member > 0.0, ranking, -1.0)
    depth = lax.broadcasted_iota(jnp.int32, (n, cap, tok), 1).astype(F32)
    pick = jnp.where(depth == ranking[:, None, :], 1.0, 0.0).reshape(slots, tok).astype(BF16)

    for v in range(parts):
        def collect(k, _):
            s = lax.rem(me - k + n, n)
            block = back.at[rows(s), piece(v)]
            send(block, block, bs, br.at[v, s], {"sp": s}).wait_recv()
            return 0

        lax.fori_loop(1, n, collect, 0)
        total = lax.dot_general(pick, back[:, piece(v)], ROWDIMS, preferred_element_type=F32)
        spread = q // parts
        fields = lambda t: pl.ds(pl.multiple_of(t * q + v * spread, spread), spread)
        out[:, fields(j)] = total.astype(BF16)
        mine = out.at[:, fields(j)]
        for p in range(1, m):
            send(mine, mine, gs.at[p], gr.at[v, p], {"tp": lax.rem(j + p, m)}).start()
    def share_of(i):
        part = slab // size(i)
        return pl.ds(pl.multiple_of((lower if i == 0 else upper) * part, part), part)

    def start_blocks(i, v):
        part = slab // size(i)
        own = lower if i == 0 else upper

        def start(k, _):
            to = lax.rem(me + k, n)
            last = lax.div(lax.rem(to * slab, q) + slab - 1, q // parts)
            block = pl.ds(pl.multiple_of(to * slab + own * part, part), part)

            @pl.when(last == v)
            def _():
                send(mix_t.at[block], got.at[me, share_of(i)], ms, mr.at[me], {"sp": to}).start()

            return 0

        lax.fori_loop(1, n, start, 0)

    for v in range(parts):
        spread = q // parts
        fields = lambda t: pl.ds(pl.multiple_of(t * q + v * spread, spread), spread)
        for p in range(1, m):
            far = lax.rem(j - p + m, m)
            theirs = out.at[:, fields(far)]
            send(theirs, theirs, gs.at[p], gr.at[v, p], {"tp": far}).wait_recv()
        for t in range(m):
            f = pl.ds(t * q + v * spread, spread)
            most = co[toks(me), f].astype(F32) + root * (gnv[:, f] * out[:, f].astype(F32))
            mix_t[f, :] = most.T.astype(BF16)

        @pl.when(par == 0)
        def _():
            start_blocks(0, v)

        @pl.when(par == 1)
        def _():
            start_blocks(1, v)

    mine = out.at[:, cols(j)]
    for p in range(1, m):
        send(mine, mine, gs.at[p], gr.at[0, p], {"tp": lax.rem(j + p, m)}).wait_send()

    scale = gnv[...]
    nhat = xo[toks(me)].astype(F32) / scale
    gained = scale * out[...].astype(F32)
    stat = jnp.mean(gained * nhat, axis=1, keepdims=True)
    mixed = co[toks(me)].astype(F32) + root * (gained - nhat * stat)
    stats[me] = jnp.broadcast_to(root * stat, (tok, 128)).T[0:8]

    def start_stats(k, _):
        to = lax.rem(me + k, n)
        send(stats.at[me], stats.at[me], ws, wr.at[me], {"sp": to}).start()
        return 0

    lax.fori_loop(1, n, start_stats, 0)

    def pass_block(i, s):
        block = got.at[s, share_of(i)]
        send(block, block, ms, mr.at[s], {"sp": s}).wait_recv()
        for p in range(1, size(i)):
            send(block, block, us.at[i], ur.at[s], {"tp": near(i, p, 0)}).start()

    def end_block(i, s):
        if size(i) > 1:
            block = got.at[s, pl.ds(0, slab // size(i) * (size(i) - 1))]
            send(block, block, us.at[i], ur.at[s], {"tp": near(i, 1, 0)}).wait_recv()
        send(stats.at[s], stats.at[s], ws, wr.at[s], {"sp": s}).wait_recv()
        left = got[s].astype(F32) - nh_t[s, inside, :].astype(F32) * stats[s][0:1]
        gow[...] += jnp.dot(left.astype(BF16), hid_all[s], preferred_element_type=F32)

    def on_side(work, s):
        @pl.when(lax.rem(s, 2) == 0)
        def _():
            work(0, s)

        @pl.when(lax.rem(s, 2) == 1)
        def _():
            work(1, s)

    d_state = jnp.dot(mixed.astype(BF16), omv[...], preferred_element_type=F32)
    here = keep[...]
    after = jnp.where(spot < tok - 1, pltpu.roll(here, tok - 1, 0), 1.0)
    a, b = scan_rows(after, d_state, True)
    enters[me] = jnp.broadcast_to(here[0:1] * b[0:1], (8, chan))
    cum[...] = a
    loc[...] = b

    def entering(k):
        to = lax.rem(me + k, n)
        return send(enters.at[me], enters.at[me], es, er.at[k], {"sp": to})

    def start_enter(k, _):
        entering(k).start()
        return 0

    lax.fori_loop(1, n, start_enter, 0)
    left = mix_t[slabs(me)].astype(F32) - nh_t[me, inside, :].astype(F32) * stats[me][0:1]
    gow[...] = jnp.dot(left.astype(BF16), hid_all[me], preferred_element_type=F32)

    def take_hidden(k, _):
        s = lax.rem(me - k + n, n)
        send(hid, hid_all.at[s], hs, hr.at[k], {"sp": s}).wait_recv()
        return 0

    def nearby(k):
        return 2 * source(lax.div(k, 2)) + lax.rem(k + par, 2)

    def pass_blocks(k, _):
        on_side(pass_block, nearby(k))
        return 0

    def end_blocks(k, _):
        on_side(end_block, nearby(k))
        return 0

    lax.fori_loop(1, n, pass_blocks, 0)

    def take_enter(k, _):
        s = lax.rem(me - k + n, n)
        send(enters.at[s], enters.at[s], es, er.at[k], {"sp": s}).wait_recv()
        return 0

    lax.fori_loop(1, n, take_enter, 0)
    enter = jnp.zeros((1, chan), F32)
    for s in range(n - 1, -1, -1):
        enter = jnp.where(s > me, carry[s, 0:1] * enter + enters[s, 0:1], enter)
    total = loc[...] + cum[...] * enter
    inward, opened, held, kept = scin[...], admit[...], retain[...], keep[...]
    signal = riv[...].astype(F32)
    g_rec[...] = total * inward * opened
    g_in[...] = total * inward * signal * opened * (1.0 - opened)
    d_log = total * prev[...] * kept - total * opened * signal * kept * kept / inward
    g_dec[...] = d_log * (-8.0 * speed) * held * (1.0 - held)

    lax.fori_loop(1, n, take_hidden, 0)

    lax.fori_loop(1, n, end_blocks, 0)

    def flush(s, _):
        for i, o in arrays:
            @pl.when(jnp.logical_and(s <= z, z + 1 < zn))
            def _():
                line(i, o, s, True).wait_send()

            @pl.when(jnp.logical_and(s >= z, z > 0))
            def _():
                line(i, o, s, False).wait_send()

        return 0

    lax.fori_loop(0, zn, flush, 0)
    for i, o in arrays:
        part = o.at[pl.ds(0, (zn - 1) * tok), pl.ds(0, (m - 1) * q)]
        send(part, part, xs.at[i], f1r.at[i, 0], {"tp": lax.rem(j + 1, m)}).wait_send()
        part = o.at[pl.ds(0, zn * tok)]
        send(part, part, ds.at[i], dr.at[i, 0], {"sp": partner}).wait_send()
    for h in range(2):
        if size(h) > 1:
            part = st1.at[h, pl.ds(0, size(h) - 1), pl.ds(0, size(1 - h))]
            send(part, part, q1.at[h], r1.at[h, 0], {"tp": near(h, 1, 0)}).wait_send()
        if size(1 - h) > 1:
            part = st2.at[h, pl.ds(0, size(1 - h) - 1)]
            send(part, part, q2.at[h], r2.at[h, 0], {"tp": near(h, 0, 1)}).wait_send()
    to = {"sp": partner}
    others = pl.ds(0, n - 1)
    send(info.at[others], info.at[others], ns, nr.at[0], to).wait_send()
    send(carry.at[others], carry.at[others], cs, cr.at[0], to).wait_send()
    send(enters.at[others], enters.at[others], es, er.at[0], to).wait_send()
    send(stats.at[others], stats.at[others], ws, wr.at[0], to).wait_send()
    send(hid_all.at[others], hid_all.at[others], hs, hr.at[0], to).wait_send()

    def flush_blocks(i):
        part = slab // size(i)
        block = got.at[others, pl.ds(0, part)]
        send(block, block, ms, mr.at[0], to).wait_send()

    @pl.when(par == 0)
    def _():
        flush_blocks(0)

    @pl.when(par == 1)
    def _():
        flush_blocks(1)

    for i in range(2):
        if size(i) > 1:
            part = slab // size(i) * (size(i) - 1)
            half_of = got.at[pl.ds(0, zn), pl.ds(0, part)]
            less = got.at[pl.ds(0, zn - 1), pl.ds(0, part)]

            @pl.when(par == i)
            def _():
                send(less, less, us.at[i], ur.at[0], {"tp": near(i, 1, 0)}).wait_send()

            @pl.when(par != i)
            def _():
                send(half_of, half_of, us.at[i], ur.at[0], {"tp": near(i, 1, 0)}).wait_send()

    part = red.at[pl.ds(0, (n - 1) * cap)]
    send(part, part, bs, br.at[0, 0], to).wait_send()


def place_kernel(*refs):
    count = len(refs) // 2
    sems = refs[-1]
    copies = [
        pltpu.make_async_copy(refs[at], refs[count + at], sems.at[at]) for at in range(count)
    ]
    for c in copies:
        c.start()
    for c in copies:
        c.wait()


def vmem_limit(outs, scratch):
    total = 0
    held = [(s.shape, s.dtype) for s in scratch if s.dtype in (F32, BF16, jnp.int32)]
    for shape, kind in list(outs) + held:
        size = -(-shape[-1] // 128) * 128 * -(-shape[-2] // 8) * 8 * jnp.dtype(kind).itemsize
        for d in shape[:-2]:
            size *= d
        total += size
    return min(VMEM_LIMIT, total + SPARE)


def shards(
    cotangent,
    normed,
    inverse_root_mean_square,
    expert_norm_scale,
    routes,
    route_probability_weight,
    gate_weight,
    up_weight,
    down_weight,
    recurrence_input,
    recurrence_gate_logits,
    input_gate_logits,
    channel_decay_weight,
    extra_log_decay,
    output_matrix,
):
    tok, feats = normed.shape
    n, m = lax.axis_size("sp"), lax.axis_size("tp")
    picks = routes.shape[1]
    cap = 2 * picks * tok // n
    slots = n * cap
    q = feats // m
    ff = gate_weight.shape[2]
    chan = recurrence_input.shape[1]
    zn = n // 2
    wide = max(sides(m))
    dma = pltpu.SemaphoreType.DMA
    vmem = lambda *s: pltpu.VMEM(s, F32)
    half = lambda *s: pltpu.VMEM(s, BF16)
    outs = [
        ((1, feats, ff), BF16),
        ((1, feats, ff), BF16),
        ((1, ff, feats), BF16),
        ((feats // n, chan), F32),
        ((tok, chan), F32),
        ((tok, chan), F32),
        ((tok, chan), F32),
    ]
    scratch = [
        half(n * tok, feats),
        half(n * tok, feats),
        pltpu.VMEM((picks, tok), jnp.int32),
        vmem(picks, tok),
        vmem(1, tok),
        vmem(1, feats),
        half(tok, chan),
        half(tok, chan),
        half(tok, chan),
        vmem(1, chan),
        vmem(tok, chan),
        half(feats, chan),
        half(feats, ff),
        half(feats, ff),
        half(ff, feats),
        vmem(n, 8, tok),
        vmem(tok, chan),
        vmem(tok, chan),
        vmem(tok, chan),
        vmem(tok, chan),
        vmem(tok, chan),
        vmem(tok, chan),
        vmem(tok, chan),
        half(tok, chan),
        vmem(n, 8, chan),
        vmem(n, 8, chan),
        half(slots, feats),
        half(slots, feats),
        half(slots, ff),
        half(slots, ff),
        half(slots, ff),
        half(slots, feats),
        half(2, max(wide - 1, 1), wide, zn * cap, q),
        half(2, wide, zn * cap, q),
        half(2, max(wide - 1, 1), zn * cap, q),
        half(slots, q),
        half(slots, q),
        half(tok, feats),
        half(n, tok, chan),
        half(feats, tok),
        half(n, feats // n, tok),
        vmem(n, 8, tok),
        half(n, max(feats // n, 128), tok),
        dma((15,)),
        dma((2, 2, zn)),
        dma((2, zn)),
        dma((2,)),
        dma((2, zn)),
        dma((2, zn)),
        dma((2,)),
        dma((2, zn)),
        dma,
        dma((n,)),
        dma,
        dma((n,)),
        dma,
        dma((n,)),
        dma((2,)),
        dma((2, zn)),
        dma((2,)),
        dma((2, zn)),
        dma,
        dma((2, n)),
        dma((m,)),
        dma((2, m)),
        dma,
        dma((n,)),
        dma((2,)),
        dma((n,)),
        dma,
        dma((n,)),
        dma,
        dma((n,)),
    ]
    args = (
        normed,
        cotangent,
        routes.T,
        route_probability_weight.T,
        inverse_root_mean_square[None, :],
        expert_norm_scale[None, :],
        recurrence_input,
        recurrence_gate_logits,
        input_gate_logits,
        channel_decay_weight[None, :],
        extra_log_decay,
        output_matrix,
        gate_weight,
        up_weight,
        down_weight,
    )
    args = [pltpu.with_memory_space_constraint(a, pltpu.HBM) for a in args]
    results = pl.pallas_call(
        functools.partial(block_kernel, n, m),
        out_shape=tuple(jax.ShapeDtypeStruct(s, d) for s, d in outs),
        in_specs=[pl.BlockSpec(memory_space=pltpu.HBM)] * len(args),
        out_specs=tuple(pl.BlockSpec(memory_space=pltpu.VMEM) for _ in outs),
        scratch_shapes=scratch,
        compiler_params=pltpu.CompilerParams(
            collective_id=0, has_side_effects=True, vmem_limit_bytes=vmem_limit(outs, scratch)
        ),
    )(*args)
    return pl.pallas_call(
        place_kernel,
        out_shape=tuple(jax.ShapeDtypeStruct(s, d) for s, d in outs),
        in_specs=[pl.BlockSpec(memory_space=pltpu.VMEM)] * len(outs),
        out_specs=tuple(pl.BlockSpec(memory_space=pltpu.HBM) for _ in outs),
        scratch_shapes=[dma((len(outs),))],
        compiler_params=pltpu.CompilerParams(vmem_limit_bytes=LEAST),
    )(*results)


def solution(mesh):
    return jax.shard_map(
        shards,
        mesh=mesh,
        in_specs=(
            P("sp", None),
            P("sp", None),
            P("sp"),
            P(),
            P("sp", None),
            P("sp", None),
            P("sp", None, "tp"),
            P("sp", None, "tp"),
            P("sp", "tp", None),
            P("sp", "tp"),
            P("sp", "tp"),
            P("sp", "tp"),
            P("tp"),
            P("sp", "tp"),
            P(None, "tp"),
        ),
        out_specs=(
            P("sp", None, "tp"),
            P("sp", None, "tp"),
            P("sp", "tp", None),
            P("sp", "tp"),
            P("sp", "tp"),
            P("sp", "tp"),
            P("sp", "tp"),
        ),
        check_vma=False,
    )
```

```python
import functools

import jax
import jax.numpy as jnp
from jax import lax
from jax.experimental import pallas as pl
from jax.experimental.pallas import tpu as pltpu
from jax.sharding import PartitionSpec as P

MESH = pl.DeviceIdType.MESH
VMEM_LIMIT = 63 * 1024 * 1024
SPARE = 8 * 1024 * 1024
LEAST = 12 * 1024 * 1024
F32, BF16 = jnp.float32, jnp.bfloat16
ROWDIMS = (((0,), (0,)), ((), ()))
COLDIMS = (((1,), (1,)), ((), ()))


def sides(m):
    high = max(d for d in range(1, m + 1) if m % d == 0 and d * d <= m)
    return high, m // high


def greet(n, m, me, j):
    barrier = pltpu.get_barrier_semaphore()
    for k in range(1, n):
        pl.semaphore_signal(
            barrier, inc=1, device_id={"sp": lax.rem(me + k, n)}, device_id_type=MESH
        )
    for p in range(1, m):
        pl.semaphore_signal(
            barrier, inc=1, device_id={"tp": lax.rem(j + p, m)}, device_id_type=MESH
        )
    pl.semaphore_wait(barrier, n - 1 + m - 1)


def send(src, dst, send_sem, recv_sem, where):
    return pltpu.make_async_remote_copy(
        src_ref=src,
        dst_ref=dst,
        send_sem=send_sem,
        recv_sem=recv_sem,
        device_id=where,
        device_id_type=MESH,
    )


def scan_rows(a, b, reverse):
    rows = a.shape[0]
    place = lax.broadcasted_iota(jnp.int32, a.shape, 0)
    step = 1
    while step < rows:
        if reverse:
            known = place < rows - step
            shift = rows - step
        else:
            known = place >= step
            shift = step
        a_far = jnp.where(known, pltpu.roll(a, shift, 0), 1.0)
        b_far = jnp.where(known, pltpu.roll(b, shift, 0), 0.0)
        b = a * b_far + b
        a = a * a_far
        step *= 2
    return a, b


def softplus_of_negative(w):
    t = jnp.exp(-jnp.abs(w))
    series = jnp.zeros_like(t)
    for k in range(10, 0, -1):
        series = t * ((1.0 / k if k % 2 else -1.0 / k) + series)
    return jnp.maximum(-w, 0.0) + jnp.where(t < 0.1, series, jnp.log(1.0 + t))


def one_minus_exp(y):
    series = jnp.ones_like(y)
    for k in range(10, 1, -1):
        series = 1.0 + y * (1.0 / k) * series
    return jnp.where(y > -0.5, -y * series, 1.0 - jnp.exp(y))


def block_kernel(
    n, m,
    nrm, cot, routes, probs, irms, gain, rin, rgate, igate, decay, extra, omat, gw, uw, dw,
    ggate, gup, gdown, gow, g_rec, g_dec, g_in,
    xo, co, rtv, pbv, irv, gnv, riv, rgv, igv, dcv, exv, omv, gwv, uwv, dwv,
    info, keep, scin, admit, retain, cum, loc, prev, hid, carry, enters,
    xg, yg, gates, ups, act, dg, du, pr, st1, mid, st2, red, back, out, hid_all, mix_t, got, stats, nh_t,
    ld, zs, zr, xs, f1r, f2r, ds, dr, ns, nr, cs, cr, hs, hr, q1, r1, q2, r2, bs, br,
    gs, gr, ms, mr, us, ur, es, er, ws, wr,
):
    me, j = lax.axis_index("sp"), lax.axis_index("tp")
    tok, feats = nrm.shape
    slots = pr.shape[0]
    cap, q = slots // n, feats // m
    chan, ff = keep.shape[1], gwv.shape[1]
    zn = n // 2
    z, par = lax.div(me, 2), lax.rem(me, 2)
    partner = me + 1 - 2 * par
    high, low = sides(m)
    upper, lower = lax.div(j, low), lax.rem(j, low)
    toks = lambda s: pl.ds(pl.multiple_of(s * tok, tok), tok)
    rows = lambda s: pl.ds(pl.multiple_of(s * cap, cap), cap)
    rows2 = lambda s: pl.ds(pl.multiple_of(s * 2 * cap, 2 * cap), 2 * cap)
    cols = lambda t: pl.ds(pl.multiple_of(t * q, q), q)
    arrays = ((0, xo), (1, co))

    def size(i):
        return low if i == 0 else high

    def near(i, along, across):
        up, down = (across, along) if i == 0 else (along, across)
        return lax.rem(upper + up, high) * low + lax.rem(lower + down, low)

    def source(k):
        fewer = jnp.minimum(z, zn - 1 - z)
        paired = k <= 2 * fewer
        d = jnp.where(paired, lax.div(k + 1, 2), k - fewer)
        odd = lax.rem(k, 2)
        down = jnp.where(paired, odd, jnp.where(z > zn - 1 - z, 1, 0))
        return z + d - 2 * d * down

    loads = [
        pltpu.make_async_copy(src, dst, ld.at[at])
        for at, (src, dst) in enumerate(
            (
                (routes, rtv),
                (probs, pbv),
                (nrm, xo.at[toks(me)]),
                (cot, co.at[toks(me)]),
                (rgate, rgv),
                (decay, dcv),
                (extra, exv),
                (igate, igv),
                (rin, riv),
                (gw.at[0], gwv),
                (uw.at[0], uwv),
                (dw.at[0], dwv),
                (omat, omv),
                (gain, gnv),
                (irms, irv),
            )
        )
    ]
    for c in loads:
        c.start()
    greet(n, m, me, j)
    loads[0].wait()
    loads[1].wait()
    info[me] = jnp.concatenate(
        [rtv[...].astype(F32), pbv[...], jnp.zeros((4, tok), F32)], axis=0
    )

    def told(k):
        to = lax.rem(me + k, n)
        return send(info.at[me], info.at[me], ns, nr.at[me], {"sp": to})

    def tell(k, _):
        told(k).start()
        return 0

    lax.fori_loop(1, n, tell, 0)

    loads[2].wait()
    loads[3].wait()

    def line(i, o, s, up):
        block = o.at[toks(2 * s + par), cols(j)]
        to = me + 2 if up else me - 2
        return send(block, block, zs.at[i, int(up), s], zr.at[i, s], {"sp": to})

    for i, o in arrays:
        @pl.when(z + 1 < zn)
        def _():
            line(i, o, z, True).start()

        @pl.when(z > 0)
        def _():
            line(i, o, z, False).start()

    def across(i, o, s):
        block = o.at[toks(2 * s + par)]
        return send(block, block, ds.at[i], dr.at[i, s], {"sp": partner})

    for i, o in arrays:
        across(i, o, z).start()

    for at in range(4, 9):
        loads[at].wait()
    speed = softplus_of_negative(dcv[...])
    retain[...] = jax.nn.sigmoid(rgv[...].astype(F32))
    admit[...] = jax.nn.sigmoid(igv[...].astype(F32))
    log_keep = -8.0 * retain[...] * speed + exv[...]
    keep[...] = jnp.exp(log_keep)
    scin[...] = jnp.sqrt(one_minus_exp(2.0 * log_keep))
    a, b = scan_rows(keep[...], scin[...] * admit[...] * riv[...].astype(F32), False)
    cum[...] = a
    loc[...] = b
    carry[me] = jnp.concatenate(
        [a[tok - 1 : tok], b[tok - 1 : tok], jnp.zeros((6, chan), F32)], axis=0
    )

    def carried(k):
        to = lax.rem(me + k, n)
        return send(carry.at[me], carry.at[me], cs, cr.at[k], {"sp": to})

    def start_carry(k, _):
        carried(k).start()
        return 0

    lax.fori_loop(1, n, start_carry, 0)

    earlier = (
        lax.broadcasted_iota(jnp.int32, (tok, tok), 0)
        < lax.broadcasted_iota(jnp.int32, (tok, tok), 1)
    ).astype(F32).astype(BF16)

    def place(s):
        @pl.when(s != me)
        def _():
            send(info.at[s], info.at[s], ns, nr.at[s], {"sp": s}).wait_recv()

        mine = info[s]
        first, second = mine[0:1] == me.astype(F32), mine[1:2] == me.astype(F32)
        member = jnp.where(jnp.logical_or(first, second), 1.0, 0.0)
        wide = jnp.broadcast_to(member, (8, tok))
        ranking = jnp.dot(wide.astype(BF16), earlier, preferred_element_type=F32)
        weight = jnp.where(first, mine[2:3], 0.0) + jnp.where(second, mine[3:4], 0.0)
        return jnp.where(member > 0.0, ranking[0:1], -1.0), weight

    for at in range(9, 15):
        loads[at].wait()

    def beside(s, i, o, t):
        block = o.at[toks(2 * s + par), cols(t)]
        send(block, block, ds.at[i], dr.at[i, s], {"sp": partner}).start()

    def onward(s, i, o):
        block = o.at[toks(2 * s + par), cols(j)]
        beside(s, i, o, j)
        for p in range(1, size(i)):
            send(block, block, xs.at[i], f1r.at[i, s], {"tp": near(i, p, 0)}).start()
        for p in range(1, size(1 - i)):
            send(block, block, xs.at[i], f2r.at[i, s], {"tp": near(i, 0, p)}).start()

    def several(o, s, count):
        return o.at[toks(2 * s + par), pl.ds(0, count * q)]

    def relayed(s):
        for i, o in arrays:
            if size(i) > 1:
                part = several(o, s, size(i) - 1)
                send(part, part, xs.at[i], f1r.at[i, s], {"tp": near(i, 1, 0)}).wait_recv()
            for c in range(1, size(i)):
                block = o.at[toks(2 * s + par), cols(near(i, size(i) - c, 0))]
                beside(s, i, o, near(i, size(i) - c, 0))
                for p in range(1, size(1 - i)):
                    send(block, block, xs.at[i], f2r.at[i, s], {"tp": near(i, 0, p)}).start()

    def whole(s):
        for i, o in arrays:
            if size(1 - i) > 1:
                part = several(o, s, m - size(i))
                send(part, part, xs.at[i], f2r.at[i, s], {"tp": near(i, 0, 1)}).wait_recv()
            for c in range(1, size(1 - i)):
                for p in range(size(i)):
                    beside(s, i, o, near(i, p, c))

    span = min(feats, 512)
    unit = min(ff, 256)

    def compute(s):
        other = 2 * s + 1 - par

        def arrive(i, o):
            block = o.at[toks(other)]
            send(block, block, ds.at[i], dr.at[i, s], {"sp": partner}).wait_recv()

        (low_at, low_weight), (high_at, high_weight) = place(2 * s), place(2 * s + 1)
        high_at = jnp.where(high_at >= 0.0, high_at + float(cap), -1.0)
        at = jnp.concatenate([low_at, high_at], axis=1)
        weight = jnp.concatenate([low_weight, high_weight], axis=1)
        here = lax.broadcasted_iota(jnp.int32, (2 * cap, 2 * tok), 0).astype(F32)
        hit = here == at
        one = jnp.where(hit, 1.0, 0.0)
        share = jnp.sum(jnp.where(hit, weight, 0.0), axis=1, keepdims=True)
        one = one.astype(BF16)
        pair = pl.ds(pl.multiple_of(s * 2 * tok, 2 * tok), 2 * tok)
        land = rows2(s)
        arrive(0, xo)
        for t in range(feats // span):
            f = pl.ds(t * span, span)
            xg[land, f] = jnp.dot(one, xo[pair, f], preferred_element_type=F32).astype(BF16)
        for t in range(ff // unit):
            f = pl.ds(t * unit, unit)
            gates[:, f] = jnp.dot(xg[land, :], gwv[:, f], preferred_element_type=F32)
            ups[:, f] = jnp.dot(xg[land, :], uwv[:, f], preferred_element_type=F32)
        arrive(1, co)
        for t in range(feats // span):
            f = pl.ds(t * span, span)
            yg[land, f] = (share * jnp.dot(one, co[pair, f], preferred_element_type=F32)).astype(
                BF16
            )
        for t in range(ff // unit):
            f = pl.ds(t * unit, unit)
            gate, up = gates[:, f], ups[:, f]
            d_act = lax.dot_general(yg[land, :], dwv[f, :], COLDIMS, preferred_element_type=F32)
            sigma = jax.nn.sigmoid(gate)
            swish = gate * sigma
            act[land, f] = (swish * up).astype(BF16)
            dg[land, f] = (d_act * up * sigma * (1.0 + gate * (1.0 - sigma))).astype(BF16)
            du[land, f] = (d_act * swish).astype(BF16)
        for t in range(feats // span):
            f = pl.ds(t * span, span)
            part = lax.dot_general(dg[land, :], gwv[f, :], COLDIMS, preferred_element_type=F32)
            part += lax.dot_general(du[land, :], uwv[f, :], COLDIMS, preferred_element_type=F32)
            pr[land, f] = part.astype(BF16)

    parts = 2 if q % 256 == 0 else 1
    piece = lambda v: pl.ds(v * (q // parts), q // parts)

    def shipped(s, v):
        return send(
            red.at[rows(s), piece(v)], back.at[rows(me), piece(v)], bs, br.at[v, me], {"sp": s}
        )

    def half_sums(s):
        for h in range(2):
            for p in range(1, size(h)):
                for c in range(size(1 - h)):
                    send(
                        pr.at[rows(2 * s + h), cols(near(h, p, c))],
                        st1.at[h, p - 1, c, rows(s)],
                        q1.at[h],
                        r1.at[h, s],
                        {"tp": near(h, p, 0)},
                    ).start()

    def middle(s):
        for h in range(2):
            if size(h) > 1:
                part = st1.at[h, pl.ds(0, size(h) - 1), pl.ds(0, size(1 - h)), rows(s)]
                send(part, part, q1.at[h], r1.at[h, s], {"tp": near(h, 1, 0)}).wait_recv()
            for c in range(size(1 - h)):
                total = pr[rows(2 * s + h), cols(near(h, 0, c))].astype(F32)
                for p in range(1, size(h)):
                    total = total + st1[h, p - 1, c, rows(s)].astype(F32)
                mid[h, c, rows(s)] = total.astype(BF16)
            for c in range(1, size(1 - h)):
                send(
                    mid.at[h, c, rows(s)],
                    st2.at[h, c - 1, rows(s)],
                    q2.at[h],
                    r2.at[h, s],
                    {"tp": near(h, 0, c)},
                ).start()

    def reduce(s):
        for h in range(2):
            if size(1 - h) > 1:
                part = st2.at[h, pl.ds(0, size(1 - h) - 1), rows(s)]
                send(part, part, q2.at[h], r2.at[h, s], {"tp": near(h, 0, 1)}).wait_recv()
            total = mid[h, 0, rows(s)].astype(F32)
            for c in range(1, size(1 - h)):
                total = total + st2[h, c - 1, rows(s)].astype(F32)
            red[rows(2 * s + h)] = total.astype(BF16)
        for v in range(parts):
            for h in range(2):
                @pl.when(2 * s + h != me)
                def _():
                    shipped(2 * s + h, v).start()

    spot = lax.broadcasted_iota(jnp.int32, (tok, chan), 0)

    def hidden():
        def take_carry(k, _):
            s = lax.rem(me - k + n, n)
            send(carry.at[s], carry.at[s], cs, cr.at[k], {"sp": s}).wait_recv()
            return 0

        lax.fori_loop(1, n, take_carry, 0)
        state = jnp.zeros((1, chan), F32)
        for s in range(n):
            state = jnp.where(s < me, carry[s, 0:1] * state + carry[s, 1:2], state)
        states = loc[...] + cum[...] * state
        hid[...] = states.astype(BF16)
        prev[...] = jnp.where(spot >= 1, pltpu.roll(states, 1, 0), state)
        hid_all[me] = hid[...]

    def share_hidden(k, _):
        to = lax.rem(me + k, n)
        send(hid, hid_all.at[me], hs, hr.at[k], {"sp": to}).start()
        return 0


    def passing(s):
        return jnp.where(s < z, jnp.where(z + 1 < zn, 1, 0), jnp.where(z > 0, 1, 0))

    def take_line(s, i, o):
        line(i, o, s, True).wait_recv()

        @pl.when(jnp.logical_and(s < z, z + 1 < zn))
        def _():
            line(i, o, s, True).start()

        @pl.when(jnp.logical_and(s > z, z > 0))
        def _():
            line(i, o, s, False).start()

    turn = jnp.where(jnp.logical_or(z == 0, z == zn - 1), 1, 2)

    def gather(k, _):
        s = source(k)
        passes = passing(s)
        late = jnp.logical_and(k >= 3, passes == 1)

        @pl.when(jnp.logical_and(k >= 3, passes == 0))
        def _():
            relayed(source(k - 2))

        for i, o in arrays:
            take_line(s, i, o)

            @pl.when(jnp.logical_not(late))
            def _():
                onward(s, i, o)

        @pl.when(late)
        def _():
            relayed(source(k - 2))

            @pl.when(k == zn - 1)
            def _():
                relayed(source(k - 1))

            for i, o in arrays:
                onward(s, i, o)

        @pl.when(k == turn)
        def _():
            compute(z)

        return 0

    lax.fori_loop(1, zn, gather, 0)
    hidden()

    @pl.when(passing(source(zn - 1)) == 0)
    def _():
        relayed(source(zn - 2))

    def middles(g, _):
        middle(source(g))
        return 0

    def reduces(g, _):
        reduce(source(g))
        return 0

    def experts(k, _):
        @pl.when(k > 1)
        def _():
            whole(source(k - 1))

        @pl.when(k == zn - 1)
        def _():
            relayed(source(k))

            def early(g, _):
                half_sums(source(g))
                return 0

            lax.fori_loop(0, zn - 2, early, 0)

        @pl.when(k == zn)
        def _():
            lax.fori_loop(1, n, share_hidden, 0)

        @pl.when(k > 1)
        def _():
            compute(source(k - 1))

        @pl.when(k == zn)
        def _():
            lax.fori_loop(0, zn - 2, middles, 0)

        @pl.when(k >= zn - 1)
        def _():
            half_sums(source(k - 1))

        return 0

    lax.fori_loop(1, zn + 1, experts, 0)
    middle(source(zn - 2))

    def wide_grads(t, _):
        f = pl.ds(pl.multiple_of(t * 256, 256), 256)
        rowsof = xg[:, f]
        ggate[0, f, :] = lax.dot_general(
            rowsof, dg[...], ROWDIMS, preferred_element_type=F32
        ).astype(BF16)
        gup[0, f, :] = lax.dot_general(
            rowsof, du[...], ROWDIMS, preferred_element_type=F32
        ).astype(BF16)
        return 0

    lax.fori_loop(0, zn - 2, reduces, 0)
    for t in range(ff // min(ff, 128)):
        f = pl.ds(t * min(ff, 128), min(ff, 128))
        gdown[0, f, :] = lax.dot_general(
            act[:, f], yg[...], ROWDIMS, preferred_element_type=F32
        ).astype(BF16)
    middle(source(zn - 1))
    lax.fori_loop(0, feats // 512, wide_grads, 0)
    reduce(source(zn - 2))
    reduce(source(zn - 1))
    back[rows(me)] = red[rows(me)]
    lax.fori_loop(feats // 512, feats // 256, wide_grads, 0)

    slab = feats // n
    slabs = lambda s: pl.ds(pl.multiple_of(s * slab, slab), slab)
    window = nh_t.shape[1]
    base = lax.div(me * slab, window)
    band = pl.ds(pl.multiple_of(base * window, window), window)
    inside = pl.ds(pl.multiple_of(me * slab - base * window, slab), slab)

    def turned(s, _):
        nh_t[s] = (xo[toks(s), band].astype(F32) / gnv[:, band]).T.astype(BF16)
        return 0

    lax.fori_loop(0, n, turned, 0)
    root = jnp.broadcast_to(irv[...], (8, tok)).T[:, 0:1]

    own = info[me]
    experts = lax.broadcasted_iota(jnp.int32, (n, tok), 0).astype(F32)
    member = jnp.where(jnp.logical_or(own[0:1] == experts, own[1:2] == experts), 1.0, 0.0)
    ranking = jnp.dot(member.astype(BF16), earlier, preferred_element_type=F32)
    ranking = jnp.where(member > 0.0, ranking, -1.0)
    depth = lax.broadcasted_iota(jnp.int32, (n, cap, tok), 1).astype(F32)
    pick = jnp.where(depth == ranking[:, None, :], 1.0, 0.0).reshape(slots, tok).astype(BF16)

    for v in range(parts):
        def collect(k, _):
            s = lax.rem(me - k + n, n)
            block = back.at[rows(s), piece(v)]
            send(block, block, bs, br.at[v, s], {"sp": s}).wait_recv()
            return 0

        lax.fori_loop(1, n, collect, 0)
        total = lax.dot_general(pick, back[:, piece(v)], ROWDIMS, preferred_element_type=F32)
        spread = q // parts
        fields = lambda t: pl.ds(pl.multiple_of(t * q + v * spread, spread), spread)
        out[:, fields(j)] = total.astype(BF16)
        mine = out.at[:, fields(j)]
        for p in range(1, m):
            send(mine, mine, gs.at[p], gr.at[v, p], {"tp": lax.rem(j + p, m)}).start()
    def share_of(i):
        part = slab // size(i)
        return pl.ds(pl.multiple_of((lower if i == 0 else upper) * part, part), part)

    def start_blocks(i, v):
        part = slab // size(i)
        own = lower if i == 0 else upper

        def start(k, _):
            to = lax.rem(me + k, n)
            last = lax.div(lax.rem(to * slab, q) + slab - 1, q // parts)
            block = pl.ds(pl.multiple_of(to * slab + own * part, part), part)

            @pl.when(last == v)
            def _():
                send(mix_t.at[block], got.at[me, share_of(i)], ms, mr.at[me], {"sp": to}).start()

            return 0

        lax.fori_loop(1, n, start, 0)

    for v in range(parts):
        spread = q // parts
        fields = lambda t: pl.ds(pl.multiple_of(t * q + v * spread, spread), spread)
        for p in range(1, m):
            far = lax.rem(j - p + m, m)
            theirs = out.at[:, fields(far)]
            send(theirs, theirs, gs.at[p], gr.at[v, p], {"tp": far}).wait_recv()
        for t in range(m):
            f = pl.ds(t * q + v * spread, spread)
            most = co[toks(me), f].astype(F32) + root * (gnv[:, f] * out[:, f].astype(F32))
            mix_t[f, :] = most.T.astype(BF16)

        @pl.when(par == 0)
        def _():
            start_blocks(0, v)

        @pl.when(par == 1)
        def _():
            start_blocks(1, v)

    mine = out.at[:, cols(j)]
    for p in range(1, m):
        send(mine, mine, gs.at[p], gr.at[0, p], {"tp": lax.rem(j + p, m)}).wait_send()

    scale = gnv[...]
    nhat = xo[toks(me)].astype(F32) / scale
    gained = scale * out[...].astype(F32)
    stat = jnp.mean(gained * nhat, axis=1, keepdims=True)
    mixed = co[toks(me)].astype(F32) + root * (gained - nhat * stat)
    stats[me] = jnp.broadcast_to(root * stat, (tok, 128)).T[0:8]

    def start_stats(k, _):
        to = lax.rem(me + k, n)
        send(stats.at[me], stats.at[me], ws, wr.at[me], {"sp": to}).start()
        return 0

    lax.fori_loop(1, n, start_stats, 0)

    def pass_block(i, s):
        block = got.at[s, share_of(i)]
        send(block, block, ms, mr.at[s], {"sp": s}).wait_recv()
        for p in range(1, size(i)):
            send(block, block, us.at[i], ur.at[s], {"tp": near(i, p, 0)}).start()

    def end_block(i, s):
        if size(i) > 1:
            block = got.at[s, pl.ds(0, slab // size(i) * (size(i) - 1))]
            send(block, block, us.at[i], ur.at[s], {"tp": near(i, 1, 0)}).wait_recv()
        send(stats.at[s], stats.at[s], ws, wr.at[s], {"sp": s}).wait_recv()
        left = got[s].astype(F32) - nh_t[s, inside, :].astype(F32) * stats[s][0:1]
        gow[...] += jnp.dot(left.astype(BF16), hid_all[s], preferred_element_type=F32)

    def on_side(work, s):
        @pl.when(lax.rem(s, 2) == 0)
        def _():
            work(0, s)

        @pl.when(lax.rem(s, 2) == 1)
        def _():
            work(1, s)

    d_state = jnp.dot(mixed.astype(BF16), omv[...], preferred_element_type=F32)
    here = keep[...]
    after = jnp.where(spot < tok - 1, pltpu.roll(here, tok - 1, 0), 1.0)
    a, b = scan_rows(after, d_state, True)
    enters[me] = jnp.broadcast_to(here[0:1] * b[0:1], (8, chan))
    cum[...] = a
    loc[...] = b

    def entering(k):
        to = lax.rem(me + k, n)
        return send(enters.at[me], enters.at[me], es, er.at[k], {"sp": to})

    def start_enter(k, _):
        entering(k).start()
        return 0

    lax.fori_loop(1, n, start_enter, 0)
    left = mix_t[slabs(me)].astype(F32) - nh_t[me, inside, :].astype(F32) * stats[me][0:1]
    gow[...] = jnp.dot(left.astype(BF16), hid_all[me], preferred_element_type=F32)

    def take_hidden(k, _):
        s = lax.rem(me - k + n, n)
        send(hid, hid_all.at[s], hs, hr.at[k], {"sp": s}).wait_recv()
        return 0

    def nearby(k):
        return 2 * source(lax.div(k, 2)) + lax.rem(k + par, 2)

    def pass_blocks(k, _):
        on_side(pass_block, nearby(k))
        return 0

    def end_blocks(k, _):
        on_side(end_block, nearby(k))
        return 0

    lax.fori_loop(1, n, pass_blocks, 0)

    def take_enter(k, _):
        s = lax.rem(me - k + n, n)
        send(enters.at[s], enters.at[s], es, er.at[k], {"sp": s}).wait_recv()
        return 0

    lax.fori_loop(1, n, take_enter, 0)
    enter = jnp.zeros((1, chan), F32)
    for s in range(n - 1, -1, -1):
        enter = jnp.where(s > me, carry[s, 0:1] * enter + enters[s, 0:1], enter)
    total = loc[...] + cum[...] * enter
    inward, opened, held, kept = scin[...], admit[...], retain[...], keep[...]
    signal = riv[...].astype(F32)
    g_rec[...] = total * inward * opened
    g_in[...] = total * inward * signal * opened * (1.0 - opened)
    d_log = total * prev[...] * kept - total * opened * signal * kept * kept / inward
    g_dec[...] = d_log * (-8.0 * speed) * held * (1.0 - held)

    lax.fori_loop(1, n, take_hidden, 0)

    lax.fori_loop(1, n, end_blocks, 0)

    def flush(s, _):
        for i, o in arrays:
            @pl.when(jnp.logical_and(s <= z, z + 1 < zn))
            def _():
                line(i, o, s, True).wait_send()

            @pl.when(jnp.logical_and(s >= z, z > 0))
            def _():
                line(i, o, s, False).wait_send()

        return 0

    lax.fori_loop(0, zn, flush, 0)
    for i, o in arrays:
        part = o.at[pl.ds(0, (zn - 1) * tok), pl.ds(0, (m - 1) * q)]
        send(part, part, xs.at[i], f1r.at[i, 0], {"tp": lax.rem(j + 1, m)}).wait_send()
        part = o.at[pl.ds(0, zn * tok)]
        send(part, part, ds.at[i], dr.at[i, 0], {"sp": partner}).wait_send()
    for h in range(2):
        if size(h) > 1:
            part = st1.at[h, pl.ds(0, size(h) - 1), pl.ds(0, size(1 - h))]
            send(part, part, q1.at[h], r1.at[h, 0], {"tp": near(h, 1, 0)}).wait_send()
        if size(1 - h) > 1:
            part = st2.at[h, pl.ds(0, size(1 - h) - 1)]
            send(part, part, q2.at[h], r2.at[h, 0], {"tp": near(h, 0, 1)}).wait_send()
    to = {"sp": partner}
    others = pl.ds(0, n - 1)
    send(info.at[others], info.at[others], ns, nr.at[0], to).wait_send()
    send(carry.at[others], carry.at[others], cs, cr.at[0], to).wait_send()
    send(enters.at[others], enters.at[others], es, er.at[0], to).wait_send()
    send(stats.at[others], stats.at[others], ws, wr.at[0], to).wait_send()
    send(hid_all.at[others], hid_all.at[others], hs, hr.at[0], to).wait_send()

    def flush_blocks(i):
        part = slab // size(i)
        block = got.at[others, pl.ds(0, part)]
        send(block, block, ms, mr.at[0], to).wait_send()

    @pl.when(par == 0)
    def _():
        flush_blocks(0)

    @pl.when(par == 1)
    def _():
        flush_blocks(1)

    for i in range(2):
        if size(i) > 1:
            part = slab // size(i) * (size(i) - 1)
            half_of = got.at[pl.ds(0, zn), pl.ds(0, part)]
            less = got.at[pl.ds(0, zn - 1), pl.ds(0, part)]

            @pl.when(par == i)
            def _():
                send(less, less, us.at[i], ur.at[0], {"tp": near(i, 1, 0)}).wait_send()

            @pl.when(par != i)
            def _():
                send(half_of, half_of, us.at[i], ur.at[0], {"tp": near(i, 1, 0)}).wait_send()

    part = red.at[pl.ds(0, (n - 1) * cap)]
    send(part, part, bs, br.at[0, 0], to).wait_send()


def place_kernel(*refs):
    count = len(refs) // 2
    sems = refs[-1]
    copies = [
        pltpu.make_async_copy(refs[at], refs[count + at], sems.at[at]) for at in range(count)
    ]
    for c in copies:
        c.start()
    for c in copies:
        c.wait()


def vmem_limit(outs, scratch):
    total = 0
    held = [(s.shape, s.dtype) for s in scratch if s.dtype in (F32, BF16, jnp.int32)]
    for shape, kind in list(outs) + held:
        size = -(-shape[-1] // 128) * 128 * -(-shape[-2] // 8) * 8 * jnp.dtype(kind).itemsize
        for d in shape[:-2]:
            size *= d
        total += size
    return min(VMEM_LIMIT, total + SPARE)


def shards(
    cotangent,
    normed,
    inverse_root_mean_square,
    expert_norm_scale,
    routes,
    route_probability_weight,
    gate_weight,
    up_weight,
    down_weight,
    recurrence_input,
    recurrence_gate_logits,
    input_gate_logits,
    channel_decay_weight,
    extra_log_decay,
    output_matrix,
):
    tok, feats = normed.shape
    n, m = lax.axis_size("sp"), lax.axis_size("tp")
    picks = routes.shape[1]
    cap = 2 * picks * tok // n
    slots = n * cap
    q = feats // m
    ff = gate_weight.shape[2]
    chan = recurrence_input.shape[1]
    zn = n // 2
    wide = max(sides(m))
    dma = pltpu.SemaphoreType.DMA
    vmem = lambda *s: pltpu.VMEM(s, F32)
    half = lambda *s: pltpu.VMEM(s, BF16)
    outs = [
        ((1, feats, ff), BF16),
        ((1, feats, ff), BF16),
        ((1, ff, feats), BF16),
        ((feats // n, chan), F32),
        ((tok, chan), F32),
        ((tok, chan), F32),
        ((tok, chan), F32),
    ]
    scratch = [
        half(n * tok, feats),
        half(n * tok, feats),
        pltpu.VMEM((picks, tok), jnp.int32),
        vmem(picks, tok),
        vmem(1, tok),
        vmem(1, feats),
        half(tok, chan),
        half(tok, chan),
        half(tok, chan),
        vmem(1, chan),
        vmem(tok, chan),
        half(feats, chan),
        half(feats, ff),
        half(feats, ff),
        half(ff, feats),
        vmem(n, 8, tok),
        vmem(tok, chan),
        vmem(tok, chan),
        vmem(tok, chan),
        vmem(tok, chan),
        vmem(tok, chan),
        vmem(tok, chan),
        vmem(tok, chan),
        half(tok, chan),
        vmem(n, 8, chan),
        vmem(n, 8, chan),
        half(slots, feats),
        half(slots, feats),
        vmem(2 * cap, ff),
        vmem(2 * cap, ff),
        half(slots, ff),
        half(slots, ff),
        half(slots, ff),
        half(slots, feats),
        half(2, max(wide - 1, 1), wide, zn * cap, q),
        half(2, wide, zn * cap, q),
        half(2, max(wide - 1, 1), zn * cap, q),
        half(slots, q),
        half(slots, q),
        half(tok, feats),
        half(n, tok, chan),
        half(feats, tok),
        half(n, feats // n, tok),
        vmem(n, 8, tok),
        half(n, max(feats // n, 128), tok),
        dma((15,)),
        dma((2, 2, zn)),
        dma((2, zn)),
        dma((2,)),
        dma((2, zn)),
        dma((2, zn)),
        dma((2,)),
        dma((2, zn)),
        dma,
        dma((n,)),
        dma,
        dma((n,)),
        dma,
        dma((n,)),
        dma((2,)),
        dma((2, zn)),
        dma((2,)),
        dma((2, zn)),
        dma,
        dma((2, n)),
        dma((m,)),
        dma((2, m)),
        dma,
        dma((n,)),
        dma((2,)),
        dma((n,)),
        dma,
        dma((n,)),
        dma,
        dma((n,)),
    ]
    args = (
        normed,
        cotangent,
        routes.T,
        route_probability_weight.T,
        inverse_root_mean_square[None, :],
        expert_norm_scale[None, :],
        recurrence_input,
        recurrence_gate_logits,
        input_gate_logits,
        channel_decay_weight[None, :],
        extra_log_decay,
        output_matrix,
        gate_weight,
        up_weight,
        down_weight,
    )
    args = [pltpu.with_memory_space_constraint(a, pltpu.HBM) for a in args]
    results = pl.pallas_call(
        functools.partial(block_kernel, n, m),
        out_shape=tuple(jax.ShapeDtypeStruct(s, d) for s, d in outs),
        in_specs=[pl.BlockSpec(memory_space=pltpu.HBM)] * len(args),
        out_specs=tuple(pl.BlockSpec(memory_space=pltpu.VMEM) for _ in outs),
        scratch_shapes=scratch,
        compiler_params=pltpu.CompilerParams(
            collective_id=0, has_side_effects=True, vmem_limit_bytes=vmem_limit(outs, scratch)
        ),
    )(*args)
    return pl.pallas_call(
        place_kernel,
        out_shape=tuple(jax.ShapeDtypeStruct(s, d) for s, d in outs),
        in_specs=[pl.BlockSpec(memory_space=pltpu.VMEM)] * len(outs),
        out_specs=tuple(pl.BlockSpec(memory_space=pltpu.HBM) for _ in outs),
        scratch_shapes=[dma((len(outs),))],
        compiler_params=pltpu.CompilerParams(vmem_limit_bytes=LEAST),
    )(*results)


def solution(mesh):
    return jax.shard_map(
        shards,
        mesh=mesh,
        in_specs=(
            P("sp", None),
            P("sp", None),
            P("sp"),
            P(),
            P("sp", None),
            P("sp", None),
            P("sp", None, "tp"),
            P("sp", None, "tp"),
            P("sp", "tp", None),
            P("sp", "tp"),
            P("sp", "tp"),
            P("sp", "tp"),
            P("tp"),
            P("sp", "tp"),
            P(None, "tp"),
        ),
        out_specs=(
            P("sp", None, "tp"),
            P("sp", None, "tp"),
            P("sp", "tp", None),
            P("sp", "tp"),
            P("sp", "tp"),
            P("sp", "tp"),
            P("sp", "tp"),
        ),
        check_vma=False,
    )
```
